32 devices in a mesh: sp: 16 (over z, y, x), dp: 2 (over core).
Axes of the slice: x: 2, y: 2, z: 4, core: 2. Of those that a mesh axis runs over, the one named last changes fastest.
Arguments:
- inputs: bfloat16 [2, 2048, 2048], P('dp', 'sp'), may hold values from -6 to 6
- conv_weight: bfloat16 [4, 2048], replicated, may hold values from -3 to 3
- gate_weight: bfloat16 [2, 8, 256, 256], P(None, 'dp'), may hold values from -0.375 to 0.375
- rate_param: float32 [2048], replicated, may hold values from 4 to 12.5
- pace: float32 [2, 2048], P('dp'), may hold values from 0.5 to 30000
Outputs:
- recurrent: bfloat16 [2, 2048, 2048], P('dp', 'sp')
The draws below stay inside these ranges and needn't reach their ends.
All inputs are finite; a program needn't handle non-finite values.
Results may differ from the reference program's by a relative error of at most 0.008.
Values may be sent and summed in bfloat16 or wider, within the bound.
A program may use at most 128 MiB of HBM per device.

```python
import math
import jax
import jax.numpy as jnp
from jax import lax

TOK_DEV = 128
HEADS = 8
BLOCK = 256
CONV = 4
DR = 2048
SEQUENCE_COUNT = 2
SEQUENCE_LENGTH = 2048


def draw_rate_param(key, part):
    slow_share = 0.5
    slow_mask = jax.random.uniform(jax.random.fold_in(key, 21), (HEADS * BLOCK,), jnp.float32) < slow_share
    slow_value = jax.random.uniform(jax.random.fold_in(key, 22), (HEADS * BLOCK,), jnp.float32, 11.5, 12.5)
    fast_value = jax.random.uniform(jax.random.fold_in(key, 23), (HEADS * BLOCK,), jnp.float32, 4.0, 6.0)
    return jnp.where(slow_mask, slow_value, fast_value)


def draw_pace(key, part):
    block_count = SEQUENCE_LENGTH // TOK_DEV
    factor = jnp.exp(jax.random.uniform(jax.random.fold_in(key, 11), (SEQUENCE_COUNT, block_count), jnp.float32, math.log(0.5), math.log(2.0)))
    constant_level = jnp.repeat(factor, TOK_DEV, axis=1)
    surge_position = jax.random.randint(jax.random.fold_in(key, 12), (SEQUENCE_COUNT, 3), 0, SEQUENCE_LENGTH)
    surge_length = jax.random.uniform(jax.random.fold_in(key, 13), (SEQUENCE_COUNT, 3), jnp.float32, 6000.0, 10000.0)
    position_flags = jnp.arange(SEQUENCE_LENGTH, dtype=jnp.int32)[None, None, :] == surge_position[:, :, None]
    surge_spans = jnp.sum(jnp.where(position_flags, surge_length[:, :, None], 0.0), axis=1)
    return constant_level + surge_spans


def shard_levels(own_key, dims, split, least, largest):
    def one(axis_at, shards_of):
        draws = jax.random.uniform(jax.random.fold_in(jax.random.fold_in(own_key, 6), axis_at), (shards_of,), jnp.float32, least / len(split), largest / len(split))
        return jnp.repeat(jnp.exp(draws), dims[axis_at] // shards_of).reshape((-1,) + (1,) * (len(dims) - axis_at - 1))

    factor_of = one(*split[0])
    for cut in split[1:]:
        factor_of = factor_of * one(*cut)
    return factor_of


def bell_draw(stream_key, shape, scale, most, split=(), kind=jnp.bfloat16):
    values = jax.random.normal(stream_key, shape, jnp.float32) * scale
    if len(split) > 0:
        values = shard_levels(stream_key, shape, split, -0.22, 0.18) * values
    return jnp.clip(values, min=-most, max=most).astype(kind)


def setup_inputs(seed: int = 0) -> dict:
    keys = jax.random.split(jax.random.key(seed), 6)
    inputs = bell_draw(keys[0], (SEQUENCE_COUNT, SEQUENCE_LENGTH, DR), 1.0, 6.0, ((0, 2), (1, 16)))
    conv_weight = bell_draw(keys[1], (CONV, DR), CONV ** -0.5, 3.0)
    gate_weight = bell_draw(keys[2], (2, HEADS, BLOCK, BLOCK), BLOCK ** -0.5, 0.375, ((1, 2),))
    rate_param = draw_rate_param(jax.random.fold_in(keys[5], 71), 0)
    pace = draw_pace(jax.random.fold_in(keys[5], 71), 0)
    return {"inputs": inputs, "conv_weight": conv_weight, "gate_weight": gate_weight, "rate_param": rate_param, "pace": pace}


gate_power = 8.0

def combine(earlier, later):
    decay_e, state_e = earlier
    decay_l, state_l = later
    return (decay_e * decay_l, decay_l * state_e + state_l)

def lru_terms(pre_recur, pre_input, values, rate_col, pace_col):
    recur_gate = jax.nn.sigmoid(pre_recur.astype(jnp.float32))
    input_gate = jax.nn.sigmoid(pre_input.astype(jnp.float32))
    log_decay = -gate_power * pace_col * recur_gate * jax.nn.softplus(-rate_col)
    decay = jnp.exp(log_decay)
    drive = jnp.sqrt(-jnp.expm1(2.0 * log_decay)) * input_gate * values.astype(jnp.float32)
    return (decay, drive)

def reference(inputs, conv_weight, gate_weight, rate_param, pace):

    def one_sequence(pair):
        seq_rows, seq_pace = pair
        length = seq_rows.shape[0]
        padded = jnp.pad(seq_rows.astype(jnp.float32), ((CONV - 1, 0), (0, 0)))
        conv_taps = conv_weight.astype(jnp.float32)
        conv_out = jnp.zeros((length, seq_rows.shape[1]), jnp.float32)
        for tap in range(CONV):
            conv_out = conv_out + conv_taps[tap][None, :] * padded[tap:tap + length]
        conv_out = conv_out.astype(jnp.bfloat16)
        by_head = conv_out.reshape(length, HEADS, BLOCK).transpose(1, 0, 2)
        head_weights = gate_weight.transpose(1, 0, 2, 3)
        head_rates = rate_param.reshape(HEADS, BLOCK)

        def one_head(triple):
            head_rows, weights, rates = triple
            preact = jnp.einsum('ti,gij->gtj', head_rows.astype(jnp.float32), weights.astype(jnp.float32)).astype(jnp.bfloat16)
            decay, drive = lru_terms(preact[0], preact[1], head_rows, rates[None, :], seq_pace[:, None])
            _, state = lax.associative_scan(combine, (decay, drive), axis=0)
            return state.astype(jnp.bfloat16)
        states = lax.map(one_head, (by_head, head_weights, head_rates))
        return states.transpose(1, 0, 2).reshape(length, HEADS * BLOCK)
    return lax.map(one_sequence, (inputs, pace))
```

```python
import functools
import math

import jax
import jax.numpy as jnp
from jax import lax
from jax.experimental import pallas as pl
from jax.experimental.pallas import tpu as pltpu
from jax.sharding import PartitionSpec as P

CONV = 4
EDGE = CONV - 1
gate_power = 8.0
SUB = 8
LANES = 128
PIECE = SUB * LANES
TINY = 1.2e-38
LN2 = math.log(2.0)
SMALL = 0.015
SPLIT = 2
FIRST = 1
MESH = pl.DeviceIdType.MESH


def softplus_neg(rate):
    e = jnp.exp(-jnp.abs(rate))
    series = e * (1.0 + e * (-0.5 + e * (1.0 / 3.0 + e * (-0.25 + e * 0.2))))
    return jnp.maximum(-rate, 0.0) + jnp.where(e < 0.03, series, jnp.log(1.0 + e))


def kernel(
    nsp, ndp, heads, block,
    x_hbm, cw_hbm, w_hbm, rate_hbm, pace_hbm, out_ref,
    x, cw, w, rate, pace_row, pace_mat, pace_perm, halo,
    ends, hloc, acum, ex_h, ex_a, stage, send_buf, recv_buf, carry,
    known, load_sem, map_sem, w_send, w_recv, halo_send, halo_recv, c_send, c_recv,
):
    me = lax.axis_index("sp")
    d = lax.axis_index("dp")
    count, width = x.shape
    steps = count // SUB
    hl = heads // ndp
    pieces = width // PIECE
    per = PIECE // block
    tiles = block // LANES

    root = nsp - 1
    first = pl.multiple_of(me * count, count)
    loads = [
        pltpu.make_async_copy(x_hbm.at[0], x, load_sem),
        pltpu.make_async_copy(cw_hbm, cw, load_sem),
        pltpu.make_async_copy(rate_hbm, rate, load_sem),
        pltpu.make_async_copy(pace_hbm.at[:, pl.ds(first, count)], pace_row, load_sem),
    ]
    map_loads = [
        pltpu.make_async_copy(w_hbm.at[:, own], w.at[:, own], map_sem.at[int(own >= FIRST)])
        for own in range(hl)
    ]
    for load in loads + map_loads:
        load.start()

    recv_buf[...] = jnp.zeros_like(recv_buf)

    barrier = pltpu.get_barrier_semaphore()

    def greet(there):
        pl.semaphore_signal(barrier, inc=1, device_id={"sp": there}, device_id_type=MESH)

    @pl.loop(1, ndp)
    def _(o):
        pl.semaphore_signal(barrier, inc=1, device_id={"dp": lax.rem(d + o, ndp)}, device_id_type=MESH)

    if root > 0:

        @pl.when(me < root)
        def _():
            greet(root)

    if root > 1:

        @pl.when(me >= 2)
        def _():
            greet(me - 1)

        @pl.when(me == 0)
        def _():
            greet(1)

    @pl.when(me == 0)
    def _():
        halo[...] = jnp.zeros_like(halo)

    def tell(which, there):
        pl.semaphore_signal(known.at[which], inc=1, device_id={"sp": there}, device_id_type=MESH)

    def meet_early():
        if root > 0:

            @pl.when(me == root)
            def _():
                pl.semaphore_wait(barrier, ndp - 1 + root)
                for there in range(root):
                    tell(0, there)

            @pl.when(me == 1)
            def _():
                if root > 1:
                    pl.semaphore_wait(barrier, ndp - 1 + 2)
                tell(1, 0)

    def meet():
        if root == 0:
            pl.semaphore_wait(barrier, ndp - 1)
        else:

            @pl.when(jnp.logical_and(me != root, me != 1))
            def _():
                pl.semaphore_wait(barrier, ndp - 1 + jnp.minimum(me, 1))

    def all_in():
        if root > 0:

            @pl.when(me < root)
            def _():
                pl.semaphore_wait(known.at[0], 1)

    w_copies = []
    for slot in range(hl, heads):
        o, own = slot // hl, slot % hl
        w_copies.append(pltpu.make_async_remote_copy(
            src_ref=w.at[:, own],
            dst_ref=w.at[:, slot],
            send_sem=w_send,
            recv_sem=w_recv.at[slot - hl],
            device_id={"dp": lax.rem(d - o + ndp, ndp)},
            device_id_type=MESH,
        ))
    halo_copy = pltpu.make_async_remote_copy(
        src_ref=x.at[pl.ds(count - SUB, SUB)],
        dst_ref=halo,
        send_sem=halo_send,
        recv_sem=halo_recv,
        device_id={"sp": lax.rem(me + 1, nsp)},
        device_id_type=MESH,
    )
    meet_early()
    for load in loads:
        load.wait()

    def meet_and_send():
        meet()

        if root > 0:

            @pl.when(jnp.logical_and(me > 0, me < root))
            def _():
                halo_copy.start()

        for copy in w_copies:
            copy.start()

    def first_halo():
        if root > 0:

            @pl.when(me == 0)
            def _():
                pl.semaphore_wait(known.at[1], 1)
                halo_copy.start()

    spread = jnp.broadcast_to(pace_row[...], (LANES, count)).T
    pace_mat[...] = spread
    for j in range(steps):
        pace_perm[j] = pace_mat[pl.ds(j, SUB, stride=steps), :]

    row = lax.broadcasted_iota(jnp.int32, (count, count), 0)
    col = lax.broadcasted_iota(jnp.int32, (count, count), 1)
    gather = jnp.where(col == (row % SUB) * steps + row // SUB, 1.0, 0.0).astype(jnp.bfloat16)
    scatter = jnp.where(row == (col % SUB) * steps + col // SUB, 1.0, 0.0).astype(jnp.bfloat16)
    sub = lax.broadcasted_iota(jnp.int32, (SUB, block), 0)

    def carry_copy(piece, src, dst):
        return pltpu.make_async_remote_copy(
            src_ref=send_buf.at[piece],
            dst_ref=recv_buf.at[piece, src],
            send_sem=c_send.at[piece],
            recv_sem=c_recv.at[piece],
            device_id={"sp": dst},
            device_id_type=MESH,
        )

    def carries(piece, many):
        block = recv_buf.at[piece, pl.ds(0, many)]
        return pltpu.make_async_remote_copy(
            src_ref=block,
            dst_ref=block,
            send_sem=c_send.at[piece],
            recv_sem=c_recv.at[piece],
            device_id={"sp": root - me},
            device_id_type=MESH,
        )

    def take_halo():
        @pl.when(me > 0)
        def _():
            halo_copy.wait_recv()

    def columns(slot):
        return pl.ds(pl.multiple_of(lax.rem(d * hl + slot, heads) * block, block), block)

    def convolve(rows, here):
        taps = cw[:, here].astype(jnp.float32)
        taps = [jnp.broadcast_to(taps[k : k + 1], (SUB, block)) for k in range(CONV)]
        out = []
        for j in range(len(rows) - EDGE):
            total = taps[0] * rows[j]
            for k in range(1, CONV):
                total = total + taps[k] * rows[j + k]
            out.append(total)
        return out

    def terms(conv, slot, here, first_step):
        conv = jnp.concatenate(conv, axis=0).astype(jnp.bfloat16)
        pre_r = jnp.dot(conv, w[0, slot], preferred_element_type=jnp.float32)
        pre_i = jnp.dot(conv, w[1, slot], preferred_element_type=jnp.float32)
        values = conv.astype(jnp.float32)
        factor = softplus_neg(rate[:, here]) * (gate_power / LN2)
        factor = jnp.broadcast_to(factor, (SUB, block))
        for j in range(conv.shape[0] // SUB):
            part = slice(SUB * j, SUB * (j + 1))
            pace_j = jnp.concatenate([pace_perm[first_step + j]] * tiles, axis=1)
            r = 1.0 / (1.0 + jnp.exp(-pre_r[part]))
            i = 1.0 / (1.0 + jnp.exp(-pre_i[part]))
            q = pace_j * factor * r
            a = jnp.exp2(-q)
            c = 2.0 * LN2
            series = q * (c + q * (c**3 / 6 * q - c * c / 2))
            gain = jnp.where(q < SMALL, series, 1.0 - a * a)
            b = gain * lax.rsqrt(jnp.maximum(gain, TINY)) * i * values[part]
            yield a, b

    def scan(pairs, slot, first_step):
        h = total_a = None
        for j, (a, b) in enumerate(pairs, first_step):
            if h is None:
                h, total_a = b, a
            else:
                h = a * h + b
                total_a = total_a * a
            part = slice(SUB * j, SUB * (j + 1))
            hloc[slot, part] = h
            acum[slot, part] = total_a

    def main_slot(slot):
        here = columns(slot)
        xp = jnp.dot(gather, x[:, here], preferred_element_type=jnp.float32)
        rows = [xp[SUB * j : SUB * (j + 1)] for j in range(steps)]
        ends[slot] = jnp.concatenate(rows[steps - EDGE :] + rows[:EDGE], axis=0)
        scan(terms(convolve(rows, here), slot, here, EDGE), slot, EDGE)

    def with_halo(rows, here):
        before = halo[:, here].astype(jnp.float32)
        out = []
        for j in range(EDGE):
            edge = before[SUB - EDGE + j : SUB - EDGE + j + 1]
            out.append(jnp.where(sub == 0, jnp.broadcast_to(edge, (SUB, block)), pltpu.roll(rows[j], 1, 0)))
        return out

    def full_slot(piece, at):
        slot = piece * per + at
        here = columns(slot)
        xp = jnp.dot(gather, x[:, here], preferred_element_type=jnp.float32)
        rows = [xp[SUB * j : SUB * (j + 1)] for j in range(steps)]
        rows = with_halo(rows[steps - EDGE :], here) + rows
        scan(terms(convolve(rows, here), slot, here, 0), slot, 0)
        chunk_end = slice(SUB * (steps - 1), SUB * steps)
        totals(slot, at, hloc[slot, chunk_end], acum[slot, chunk_end])

    def edge_slot(piece, at):
        slot = piece * per + at
        here = columns(slot)
        rows = [ends[slot, SUB * j : SUB * (j + 1)] for j in range(2 * EDGE)]
        rows = with_halo(rows[:EDGE], here) + rows[EDGE:]
        conv = convolve(rows, here)
        scan(terms(conv, slot, here, 0), slot, 0)
        edge_end = slice(SUB * (EDGE - 1), SUB * EDGE)
        chunk_end = slice(SUB * (steps - 1), SUB * steps)
        h = hloc[slot, chunk_end] + acum[slot, chunk_end] * hloc[slot, edge_end]
        totals(slot, at, h, acum[slot, chunk_end] * acum[slot, edge_end])

    def totals(slot, at, h, total_a):
        for shift in (1, 2, 4):
            inside = sub >= shift
            earlier_a = jnp.where(inside, pltpu.roll(total_a, shift, 0), 1.0)
            earlier_h = jnp.where(inside, pltpu.roll(h, shift, 0), 0.0)
            h = total_a * earlier_h + h
            total_a = total_a * earlier_a
        ex_h[slot] = jnp.where(sub >= 1, pltpu.roll(h, 1, 0), 0.0)
        ex_a[slot] = jnp.where(sub >= 1, pltpu.roll(total_a, 1, 0), 1.0)
        log_a = jnp.log2(jnp.maximum(total_a, TINY))
        for t in range(tiles):
            lanes = slice(LANES * t, LANES * (t + 1))
            stage[pl.ds(at * tiles + t, 1), :] = log_a[SUB - 1 :, lanes]
            stage[pl.ds(SUB + at * tiles + t, 1), :] = h[SUB - 1 :, lanes]

    def wait_maps(low, high):
        for slot in range(max(hl, low), high):
            w_copies[slot - hl].wait_recv()

    def main_slots(low, high):
        wait_maps(low, high)

        @pl.loop(low, high, unroll=True)
        def _(slot):
            main_slot(slot)

    def edge_and_send(piece, split):
        @pl.loop(0, split, unroll=True)
        def _(at):
            edge_slot(piece, at)

        if split < per:
            wait_maps(piece * per + split, piece * per + per)

            @pl.loop(split, per, unroll=True)
            def _(at):
                full_slot(piece, at)

        send_buf[piece] = stage[...].astype(jnp.bfloat16)

        if piece == 0:
            all_in()

        @pl.loop(me + 1, nsp)
        def _(dst):
            carry_copy(piece, me, dst).start()

    half = per // 2
    for piece in range(pieces):
        low = piece * per
        if piece == 0:
            begun = low + min(hl, FIRST)
            for load in map_loads[:begun]:
                load.wait()
            middle = begun + (low + per - begun) // 2
            main_slots(low, begun)
            for load in map_loads[begun:]:
                load.wait()
            meet_and_send()
            main_slots(begun, middle)
            first_halo()
            main_slots(middle, low + per)
        else:
            ahead = SPLIT if piece == 1 else 0
            if ahead:
                main_slots(low, low + ahead)
            if piece == 1:
                take_halo()
                edge_and_send(0, per)
            edge_and_send(piece, ahead)

    def finish_slot(piece, at):
        slot = piece * per + at
        off = pl.multiple_of(lax.rem(d * hl + slot, heads) * block, block)
        start = jnp.concatenate(
            [
                jnp.broadcast_to(carry[pl.ds(at * tiles + t, 1), :], (SUB, LANES))
                for t in range(tiles)
            ],
            axis=1,
        )
        start = ex_h[slot] + ex_a[slot] * start
        edge_end = slice(SUB * (EDGE - 1), SUB * EDGE)
        later = start
        if piece == 0 or at < SPLIT:
            later = hloc[slot, edge_end] + acum[slot, edge_end] * start
        states = [
            hloc[slot, SUB * j : SUB * (j + 1)]
            + acum[slot, SUB * j : SUB * (j + 1)] * (start if j < EDGE else later)
            for j in range(steps)
        ]
        states = jnp.concatenate(states, axis=0).astype(jnp.bfloat16)
        placed = jnp.dot(scatter, states, preferred_element_type=jnp.float32)
        out_ref[0, :, pl.ds(off, block)] = placed.astype(jnp.bfloat16)

    for piece in range(pieces):

        for many in range(1, nsp):

            @pl.when(me == many)
            def _(many=many):
                carries(piece, many).wait_recv()

        start = jnp.zeros(carry.shape, jnp.float32)
        for src in range(root):
            got = recv_buf[piece, src].astype(jnp.float32)
            start = jnp.exp2(got[:SUB]) * start + got[SUB:]
        carry[...] = start

        for at in range(per):
            finish_slot(piece, at)

    for copy in w_copies:
        copy.wait_send()

    @pl.when(me < nsp - 1)
    def _():
        halo_copy.wait_send()

    for piece in range(pieces):

        for many in range(1, nsp):

            @pl.when(root - me == many)
            def _(many=many):
                carries(piece, many).wait_send()


def body(inputs, conv_weight, gate_weight, rate_param, pace):
    nsp = lax.axis_size("sp")
    ndp = lax.axis_size("dp")
    _, count, width = inputs.shape
    block = gate_weight.shape[-1]
    heads = width // block
    hl = heads // ndp
    pieces = width // PIECE
    f32, bf16 = jnp.float32, jnp.bfloat16
    hbm = pl.BlockSpec(memory_space=pltpu.HBM)
    dma = pltpu.SemaphoreType.DMA
    return pl.pallas_call(
        functools.partial(kernel, nsp, ndp, heads, block),
        out_shape=pltpu.VMEM(inputs.shape, bf16),
        in_specs=[hbm] * 5,
        out_specs=pl.BlockSpec(memory_space=pltpu.VMEM),
        scratch_shapes=[
            pltpu.VMEM((count, width), bf16),
            pltpu.VMEM(conv_weight.shape, bf16),
            pltpu.VMEM((2, heads, block, block), bf16),
            pltpu.VMEM((1, width), f32),
            pltpu.VMEM((1, count), f32),
            pltpu.VMEM((count, LANES), f32),
            pltpu.VMEM((count // SUB, SUB, LANES), f32),
            pltpu.VMEM((SUB, width), bf16),
            pltpu.VMEM((heads, 2 * EDGE * SUB, block), f32),
            pltpu.VMEM((heads, count, block), f32),
            pltpu.VMEM((heads, count, block), f32),
            pltpu.VMEM((heads, SUB, block), f32),
            pltpu.VMEM((heads, SUB, block), f32),
            pltpu.VMEM((2 * SUB, LANES), f32),
            pltpu.VMEM((pieces, 2 * SUB, LANES), bf16),
            pltpu.VMEM((pieces, nsp, 2 * SUB, LANES), bf16),
            pltpu.VMEM((SUB, LANES), f32),
            pltpu.SemaphoreType.REGULAR((2,)),
            dma,
            dma((2,)),
            dma,
            dma((heads - hl,)),
            dma,
            dma,
            dma((pieces,)),
            dma((pieces,)),
        ],
        compiler_params=pltpu.CompilerParams(collective_id=0, has_side_effects=True),
    )(inputs, conv_weight, gate_weight, rate_param.reshape(1, width), pace)


def solution(mesh):
    return jax.shard_map(
        body,
        mesh=mesh,
        in_specs=(P("dp", "sp", None), P(), P(None, "dp", None, None), P(), P("dp", None)),
        out_specs=P("dp", "sp", None),
        check_vma=False,
    )
```

```python
import functools
import math

import jax
import jax.numpy as jnp
from jax import lax
from jax.experimental import pallas as pl
from jax.experimental.pallas import tpu as pltpu
from jax.sharding import PartitionSpec as P

CONV = 4
EDGE = CONV - 1
gate_power = 8.0
SUB = 8
LANES = 128
TINY = 1.2e-38
LN2 = math.log(2.0)
LOG2E = 1.0 / LN2
SMALL = 0.015
ROW = 4
FIRST = 2
MESH = pl.DeviceIdType.MESH


def softplus_neg(rate):
    e = jnp.exp(-jnp.abs(rate))
    series = e * (1.0 + e * (-0.5 + e * (1.0 / 3.0 + e * (-0.25 + e * 0.2))))
    return jnp.maximum(-rate, 0.0) + jnp.where(e < 0.03, series, jnp.log(1.0 + e))


def kernel(
    nsp, ndp, heads, block,
    x_hbm, cw_hbm, w_hbm, rate_hbm, pace_hbm, out_ref,
    x, cw, w, rate, pace_row, pace_mat, pace_perm, last, halo,
    ends, convs, hloc, acum, ex_h, ex_a, stage, send_buf, recv_buf, carry,
    known, met, load_sem, map_sem, w_send, w_recv, halo_send, halo_recv, c_send, c_recv,
):
    me = lax.axis_index("sp")
    d = lax.axis_index("dp")
    count, width = x.shape
    steps = count // SUB
    hl = heads // ndp
    tiles = block // LANES
    lines = heads * tiles
    root = nsp - 1
    scope = jax.named_scope

    first = pl.multiple_of(me * count, count)
    loads = [
        pltpu.make_async_copy(x_hbm.at[0], x, load_sem),
        pltpu.make_async_copy(cw_hbm, cw, load_sem),
        pltpu.make_async_copy(rate_hbm, rate, load_sem),
        pltpu.make_async_copy(pace_hbm.at[:, pl.ds(first, count)], pace_row, load_sem),
    ]
    map_loads = [
        pltpu.make_async_copy(w_hbm.at[:, own], w.at[:, own], map_sem.at[int(own >= FIRST)])
        for own in range(hl)
    ]
    for load in loads + map_loads:
        load.start()

    recv_buf[...] = jnp.zeros_like(recv_buf)

    barrier = pltpu.get_barrier_semaphore()

    def greet(there):
        pl.semaphore_signal(barrier, inc=1, device_id={"sp": there}, device_id_type=MESH)

    @pl.loop(d + 1, ndp)
    def _(o):
        pl.semaphore_signal(barrier, inc=1, device_id={"dp": o}, device_id_type=MESH)

    if root > 0:

        @pl.when(me > 0)
        def _():
            greet(me - 1)

    if root > 1:

        @pl.when(me < root - 1)
        def _():
            greet(root)

        @pl.when(me == root - 1)
        def _():
            greet(root)

    @pl.when(me == 0)
    def _():
        halo[...] = jnp.zeros_like(halo)

    def meet():
        pl.semaphore_wait(barrier, d + jnp.where(me == root, root if root > 1 else 0, min(root, 1)))

    def meet_early():
        if root > 0:

            @pl.when(me == root)
            def _():
                meet()
                for there in range(root):
                    pl.semaphore_signal(known, inc=1, device_id={"sp": there}, device_id_type=MESH)

    def meet_maps():
        @pl.when(jnp.logical_and(me < max(root, 1), d > 0))
        def _():
            meet()

        @pl.loop(0, d)
        def _(o):
            pl.semaphore_signal(met, inc=1, device_id={"dp": o}, device_id_type=MESH)

        @pl.when(d < ndp - 1)
        def _():
            pl.semaphore_wait(met, ndp - 1 - d)

    def meet_halo():
        @pl.when(jnp.logical_and(me < root, d == 0))
        def _():
            meet()

    w_copies = []
    for slot in range(hl, heads):
        o, own = slot // hl, slot % hl
        w_copies.append(pltpu.make_async_remote_copy(
            src_ref=w.at[:, own],
            dst_ref=w.at[:, slot],
            send_sem=w_send,
            recv_sem=w_recv.at[slot - hl],
            device_id={"dp": lax.rem(d - o + ndp, ndp)},
            device_id_type=MESH,
        ))
    halo_copy = pltpu.make_async_remote_copy(
        src_ref=last,
        dst_ref=halo,
        send_sem=halo_send,
        recv_sem=halo_recv,
        device_id={"sp": lax.rem(me + 1, nsp)},
        device_id_type=MESH,
    )

    def carry_copy(src, dst):
        return pltpu.make_async_remote_copy(
            src_ref=send_buf,
            dst_ref=recv_buf.at[src],
            send_sem=c_send,
            recv_sem=c_recv,
            device_id={"sp": dst},
            device_id_type=MESH,
        )

    def carries(many):
        block = recv_buf.at[pl.ds(0, many)]
        return pltpu.make_async_remote_copy(
            src_ref=block,
            dst_ref=block,
            send_sem=c_send,
            recv_sem=c_recv,
            device_id={"sp": root - me},
            device_id_type=MESH,
        )

    row = lax.broadcasted_iota(jnp.int32, (count, count), 0)
    col = lax.broadcasted_iota(jnp.int32, (count, count), 1)
    gather = jnp.where(col == (row % SUB) * steps + row // SUB, 1.0, 0.0).astype(jnp.bfloat16)
    scatter = jnp.where(row == (col % SUB) * steps + col // SUB, 1.0, 0.0).astype(jnp.bfloat16)
    sub = lax.broadcasted_iota(jnp.int32, (SUB, block), 0)

    def columns(slot):
        return pl.ds(pl.multiple_of(lax.rem(d * hl + slot, heads) * block, block), block)

    def convolve(rows, here):
        taps = cw[:, here].astype(jnp.float32)
        taps = [jnp.broadcast_to(taps[k : k + 1], (SUB, block)) for k in range(CONV)]
        out = []
        for j in range(len(rows) - EDGE):
            total = taps[0] * rows[j]
            for k in range(1, CONV):
                total = total + taps[k] * rows[j + k]
            out.append(total)
        return jnp.concatenate(out, axis=0)

    def conv_main(slot):
        here = columns(slot)
        xp = jnp.dot(gather, x[:, here], preferred_element_type=jnp.float32)
        rows = [xp[SUB * j : SUB * (j + 1)] for j in range(steps)]
        ends[slot] = jnp.concatenate(rows[steps - EDGE :] + rows[:EDGE], axis=0)
        convs[slot] = convolve(rows, here)

    def conv_edge(slot):
        here = columns(slot)
        rows = [ends[slot, SUB * j : SUB * (j + 1)] for j in range(2 * EDGE)]
        before = halo[:, here].astype(jnp.float32)
        for j in range(EDGE):
            edge = before[CONV - EDGE + j : CONV - EDGE + j + 1]
            rows[j] = jnp.where(sub == 0, jnp.broadcast_to(edge, (SUB, block)), pltpu.roll(rows[j], 1, 0))
        return convolve(rows, here)

    def scan(conv, slot, first_step):
        conv = conv.astype(jnp.bfloat16)
        pre_r = jnp.dot(conv, w[0, slot], preferred_element_type=jnp.float32)
        pre_i = jnp.dot(conv, w[1, slot], preferred_element_type=jnp.float32)
        values = conv.astype(jnp.float32)
        factor = softplus_neg(rate[:, columns(slot)]) * (-gate_power / LN2)
        factor = jnp.broadcast_to(factor, (SUB, block))
        h = total_a = None
        for j in range(conv.shape[0] // SUB):
            part = slice(SUB * j, SUB * (j + 1))
            pace_j = jnp.concatenate([pace_perm[first_step + j]] * tiles, axis=1)
            r = 1.0 / (1.0 + jnp.exp2(pre_r[part] * -LOG2E))
            i = 1.0 / (1.0 + jnp.exp2(pre_i[part] * -LOG2E))
            n = pace_j * factor * r
            a = jnp.exp2(n)
            c = 2.0 * LN2
            series = n * (n * (n * (-(c**3) / 6) - c * c / 2) - c)
            gain = jnp.where(n > -SMALL, series, 1.0 - a * a)
            b = gain * lax.rsqrt(jnp.maximum(gain, TINY)) * i * values[part]
            if h is None:
                h, total_a = b, a
            else:
                h = a * h + b
                total_a = total_a * a
            place = slice(SUB * (first_step + j), SUB * (first_step + j + 1))
            hloc[slot, place] = h
            acum[slot, place] = total_a

    def main_slot(slot):
        scan(convs[slot], slot, EDGE)

    def edge_slot(slot):
        scan(conv_edge(slot), slot, 0)
        edge_end = slice(SUB * (EDGE - 1), SUB * EDGE)
        chunk_end = slice(SUB * (steps - 1), SUB * steps)
        h = hloc[slot, chunk_end] + acum[slot, chunk_end] * hloc[slot, edge_end]
        totals(slot, h, acum[slot, chunk_end] * acum[slot, edge_end])

    def totals(slot, h, total_a):
        for shift in (1, 2, 4):
            inside = sub >= shift
            earlier_a = jnp.where(inside, pltpu.roll(total_a, shift, 0), 1.0)
            earlier_h = jnp.where(inside, pltpu.roll(h, shift, 0), 0.0)
            h = total_a * earlier_h + h
            total_a = total_a * earlier_a
        ex_h[slot] = jnp.where(sub >= 1, pltpu.roll(h, 1, 0), 0.0)
        ex_a[slot] = jnp.where(sub >= 1, pltpu.roll(total_a, 1, 0), 1.0)
        log_a = jnp.log2(jnp.maximum(total_a, TINY))
        for t in range(tiles):
            lanes = slice(LANES * t, LANES * (t + 1))
            stage[pl.ds(slot * tiles + t, 1), :] = log_a[SUB - 1 :, lanes]
            stage[pl.ds(lines + slot * tiles + t, 1), :] = h[SUB - 1 :, lanes]

    with scope("meet_early"):
        meet_early()
    with scope("loads"):
        for load in loads:
            load.wait()
    last[...] = x[count - SUB :, :].astype(jnp.float32)[SUB - CONV :].astype(jnp.bfloat16)
    with scope("meet_maps"):
        meet_maps()
    with scope("maps_a"):
        for load in map_loads[:FIRST]:
            load.wait()
        for own in range(min(FIRST, hl)):
            for copy in w_copies[own::hl]:
                copy.start()

    def send_halo():
        if root > 0:

            @pl.when(me < root)
            def _():
                halo_copy.start()

    @pl.when(d > 0)
    def _():
        send_halo()

    spread = jnp.broadcast_to(pace_row[...], (LANES, count)).T
    pace_mat[...] = spread
    for j in range(steps):
        pace_perm[j] = pace_mat[pl.ds(j, SUB, stride=steps), :]

    with scope("conv_own"):
        for slot in range(hl):
            conv_main(slot)
    with scope("maps_b"):
        for load in map_loads[FIRST:]:
            load.wait()
        for own in range(FIRST, hl):
            for copy in w_copies[own::hl]:
                copy.start()
    with scope("meet_halo"):
        meet_halo()

    @pl.when(d == 0)
    def _():
        send_halo()

    with scope("own"):
        for slot in range(hl):
            main_slot(slot)
        for slot in range(hl, heads):
            conv_main(slot)
    for slot in range(hl, heads):
        with scope("map%d" % slot):
            w_copies[slot - hl].wait_recv()
        with scope("main%d" % slot):
            main_slot(slot)
    with scope("take_halo"):

        @pl.when(me > 0)
        def _():
            halo_copy.wait_recv()

    with scope("edges"):
        for slot in range(heads):
            edge_slot(slot)
        send_buf[...] = stage[...].astype(jnp.bfloat16)
    with scope("all_in"):

        @pl.when(me < root)
        def _():
            pl.semaphore_wait(known, 1)

    for rest in range(ROW):
        for dst in range(nsp - ROW + rest, 0, -ROW):

            @pl.when(me < dst)
            def _(dst=dst):
                carry_copy(me, dst).start()

    with scope("carry"):
        for many in range(1, nsp):

            @pl.when(me == many)
            def _(many=many):
                carries(many).wait_recv()

    with scope("finish"):
        start = jnp.zeros(carry.shape, jnp.float32)
        for src in range(root):
            got = recv_buf[src].astype(jnp.float32)
            start = jnp.exp2(got[:lines]) * start + got[lines:]
        carry[...] = start

        for slot in range(heads):
            start = jnp.concatenate(
                [
                    jnp.broadcast_to(carry[pl.ds(slot * tiles + t, 1), :], (SUB, LANES))
                    for t in range(tiles)
                ],
                axis=1,
            )
            start = ex_h[slot] + ex_a[slot] * start
            edge_end = slice(SUB * (EDGE - 1), SUB * EDGE)
            later = hloc[slot, edge_end] + acum[slot, edge_end] * start
            states = [
                hloc[slot, SUB * j : SUB * (j + 1)]
                + acum[slot, SUB * j : SUB * (j + 1)] * (start if j < EDGE else later)
                for j in range(steps)
            ]
            states = jnp.concatenate(states, axis=0).astype(jnp.bfloat16)
            placed = jnp.dot(scatter, states, preferred_element_type=jnp.float32)
            out_ref[0, :, columns(slot)] = placed.astype(jnp.bfloat16)

    with scope("tail"):
        for copy in w_copies:
            copy.wait_send()

        if root > 0:

            @pl.when(me < root)
            def _():
                halo_copy.wait_send()

        for many in range(1, nsp):

            @pl.when(root - me == many)
            def _(many=many):
                carries(many).wait_send()


def body(inputs, conv_weight, gate_weight, rate_param, pace):
    nsp = lax.axis_size("sp")
    ndp = lax.axis_size("dp")
    _, count, width = inputs.shape
    block = gate_weight.shape[-1]
    heads = width // block
    hl = heads // ndp
    lines = width // LANES
    f32, bf16 = jnp.float32, jnp.bfloat16
    hbm = pl.BlockSpec(memory_space=pltpu.HBM)
    dma = pltpu.SemaphoreType.DMA
    return pl.pallas_call(
        functools.partial(kernel, nsp, ndp, heads, block),
        out_shape=pltpu.VMEM(inputs.shape, bf16),
        in_specs=[hbm] * 5,
        out_specs=pl.BlockSpec(memory_space=pltpu.VMEM),
        scratch_shapes=[
            pltpu.VMEM((count, width), bf16),
            pltpu.VMEM(conv_weight.shape, bf16),
            pltpu.VMEM((2, heads, block, block), bf16),
            pltpu.VMEM((1, width), f32),
            pltpu.VMEM((1, count), f32),
            pltpu.VMEM((count, LANES), f32),
            pltpu.VMEM((count // SUB, SUB, LANES), f32),
            pltpu.VMEM((CONV, width), bf16),
            pltpu.VMEM((CONV, width), bf16),
            pltpu.VMEM((heads, 2 * EDGE * SUB, block), f32),
            pltpu.VMEM((heads, count - EDGE * SUB, block), f32),
            pltpu.VMEM((heads, count, block), f32),
            pltpu.VMEM((heads, count, block), f32),
            pltpu.VMEM((heads, SUB, block), f32),
            pltpu.VMEM((heads, SUB, block), f32),
            pltpu.VMEM((2 * lines, LANES), f32),
            pltpu.VMEM((2 * lines, LANES), bf16),
            pltpu.VMEM((nsp, 2 * lines, LANES), bf16),
            pltpu.VMEM((lines, LANES), f32),
            pltpu.SemaphoreType.REGULAR,
            pltpu.SemaphoreType.REGULAR,
            dma,
            dma((2,)),
            dma,
            dma((heads - hl,)),
            dma,
            dma,
            dma,
            dma,
        ],
        compiler_params=pltpu.CompilerParams(collective_id=0, has_side_effects=True),
    )(inputs, conv_weight, gate_weight, rate_param.reshape(1, width), pace)


def solution(mesh):
    return jax.shard_map(
        body,
        mesh=mesh,
        in_specs=(P("dp", "sp", None), P(), P(None, "dp", None, None), P(), P("dp", None)),
        out_specs=P("dp", "sp", None),
        check_vma=False,
    )
```

```python
import functools
import math

import jax
import jax.numpy as jnp
from jax import lax
from jax.experimental import pallas as pl
from jax.experimental.pallas import tpu as pltpu
from jax.sharding import PartitionSpec as P

CONV = 4
EDGE = CONV - 1
gate_power = 8.0
SUB = 8
LANES = 128
TINY = 1.2e-38
LN2 = math.log(2.0)
LOG2E = 1.0 / LN2
SMALL = 0.015
ROW = 4
FIRST = 2
MESH = pl.DeviceIdType.MESH


def softplus_neg(rate):
    e = jnp.exp(-jnp.abs(rate))
    series = e * (1.0 + e * (-0.5 + e * (1.0 / 3.0 + e * (-0.25 + e * 0.2))))
    return jnp.maximum(-rate, 0.0) + jnp.where(e < 0.03, series, jnp.log(1.0 + e))


def kernel(
    nsp, ndp, heads, block,
    x_hbm, cw_hbm, w_hbm, rate_hbm, pace_hbm, part_h, part_a, carry,
    x, cw, w, rate, pace_row, pace_mat, pace_perm, last, halo,
    ends, convs, hloc, acum, ex_h, ex_a, lay_h, lay_a, stage, send_buf, recv_buf,
    known, met, load_sem, map_sem, w_send, w_recv, halo_send, halo_recv, c_send, c_recv,
):
    me = lax.axis_index("sp")
    d = lax.axis_index("dp")
    count, width = x.shape
    steps = count // SUB
    hl = heads // ndp
    tiles = block // LANES
    lines = heads * tiles
    root = nsp - 1
    scope = jax.named_scope

    first = pl.multiple_of(me * count, count)
    loads = [
        pltpu.make_async_copy(x_hbm.at[0], x, load_sem),
        pltpu.make_async_copy(cw_hbm, cw, load_sem),
        pltpu.make_async_copy(rate_hbm, rate, load_sem),
        pltpu.make_async_copy(pace_hbm.at[:, pl.ds(first, count)], pace_row, load_sem),
    ]
    map_loads = [
        pltpu.make_async_copy(w_hbm.at[:, own], w.at[:, own], map_sem.at[int(own >= FIRST)])
        for own in range(hl)
    ]
    for load in loads + map_loads:
        load.start()

    recv_buf[...] = jnp.zeros_like(recv_buf)

    barrier = pltpu.get_barrier_semaphore()

    def greet(there):
        pl.semaphore_signal(barrier, inc=1, device_id={"sp": there}, device_id_type=MESH)

    @pl.loop(d + 1, ndp)
    def _(o):
        pl.semaphore_signal(barrier, inc=1, device_id={"dp": o}, device_id_type=MESH)

    if root > 0:

        @pl.when(me > 0)
        def _():
            greet(me - 1)

    if root > 1:

        @pl.when(me < root - 1)
        def _():
            greet(root)

        @pl.when(me == root - 1)
        def _():
            greet(root)

    @pl.when(me == 0)
    def _():
        halo[...] = jnp.zeros_like(halo)

    def meet():
        pl.semaphore_wait(barrier, d + jnp.where(me == root, root if root > 1 else 0, min(root, 1)))

    def meet_early():
        if root > 0:

            @pl.when(me == root)
            def _():
                meet()
                for there in range(root):
                    pl.semaphore_signal(known, inc=1, device_id={"sp": there}, device_id_type=MESH)

    def meet_maps():
        @pl.when(jnp.logical_and(me < max(root, 1), d > 0))
        def _():
            meet()

        @pl.loop(0, d)
        def _(o):
            pl.semaphore_signal(met, inc=1, device_id={"dp": o}, device_id_type=MESH)

        @pl.when(d < ndp - 1)
        def _():
            pl.semaphore_wait(met, ndp - 1 - d)

    def meet_halo():
        @pl.when(jnp.logical_and(me < root, d == 0))
        def _():
            meet()

    w_copies = []
    for slot in range(hl, heads):
        o, own = slot // hl, slot % hl
        w_copies.append(pltpu.make_async_remote_copy(
            src_ref=w.at[:, own],
            dst_ref=w.at[:, slot],
            send_sem=w_send,
            recv_sem=w_recv.at[slot - hl],
            device_id={"dp": lax.rem(d - o + ndp, ndp)},
            device_id_type=MESH,
        ))
    halo_copy = pltpu.make_async_remote_copy(
        src_ref=last,
        dst_ref=halo,
        send_sem=halo_send,
        recv_sem=halo_recv,
        device_id={"sp": lax.rem(me + 1, nsp)},
        device_id_type=MESH,
    )

    def carry_copy(src, dst, low=0):
        return pltpu.make_async_remote_copy(
            src_ref=send_buf.at[pl.ds(low, 2 * lines - low)],
            dst_ref=recv_buf.at[pl.ds(2 * lines * src + low, 2 * lines - low)],
            send_sem=c_send,
            recv_sem=c_recv,
            device_id={"sp": dst},
            device_id_type=MESH,
        )

    def carries(rows):
        block = recv_buf.at[pl.ds(0, rows)]
        return pltpu.make_async_remote_copy(
            src_ref=block,
            dst_ref=block,
            send_sem=c_send,
            recv_sem=c_recv,
            device_id={"sp": root - me},
            device_id_type=MESH,
        )

    row = lax.broadcasted_iota(jnp.int32, (count, count), 0)
    col = lax.broadcasted_iota(jnp.int32, (count, count), 1)
    gather = jnp.where(col == (row % SUB) * steps + row // SUB, 1.0, 0.0).astype(jnp.bfloat16)
    sub = lax.broadcasted_iota(jnp.int32, (SUB, block), 0)

    def columns(slot):
        return pl.ds(pl.multiple_of(lax.rem(d * hl + slot, heads) * block, block), block)

    def convolve(rows, here):
        taps = cw[:, here].astype(jnp.float32)
        taps = [jnp.broadcast_to(taps[k : k + 1], (SUB, block)) for k in range(CONV)]
        out = []
        for j in range(len(rows) - EDGE):
            total = taps[0] * rows[j]
            for k in range(1, CONV):
                total = total + taps[k] * rows[j + k]
            out.append(total)
        return jnp.concatenate(out, axis=0)

    def conv_main(slot):
        here = columns(slot)
        xp = jnp.dot(gather, x[:, here], preferred_element_type=jnp.float32)
        rows = [xp[SUB * j : SUB * (j + 1)] for j in range(steps)]
        ends[slot] = jnp.concatenate(rows[steps - EDGE :] + rows[:EDGE], axis=0)
        convs[slot] = convolve(rows, here)

    def conv_edge(slot):
        here = columns(slot)
        rows = [ends[slot, SUB * j : SUB * (j + 1)] for j in range(2 * EDGE)]
        before = halo[:, here].astype(jnp.float32)
        for j in range(EDGE):
            edge = before[CONV - EDGE + j : CONV - EDGE + j + 1]
            rows[j] = jnp.where(sub == 0, jnp.broadcast_to(edge, (SUB, block)), pltpu.roll(rows[j], 1, 0))
        return convolve(rows, here)

    def scan(conv, slot, first_step):
        conv = conv.astype(jnp.bfloat16)
        pre_r = jnp.dot(conv, w[0, slot], preferred_element_type=jnp.float32)
        pre_i = jnp.dot(conv, w[1, slot], preferred_element_type=jnp.float32)
        values = conv.astype(jnp.float32)
        factor = softplus_neg(rate[:, columns(slot)]) * (-gate_power / LN2)
        factor = jnp.broadcast_to(factor, (SUB, block))
        h = total_a = None
        for j in range(conv.shape[0] // SUB):
            part = slice(SUB * j, SUB * (j + 1))
            pace_j = jnp.concatenate([pace_perm[first_step + j]] * tiles, axis=1)
            r = 1.0 / (1.0 + jnp.exp2(pre_r[part] * -LOG2E))
            i = 1.0 / (1.0 + jnp.exp2(pre_i[part] * -LOG2E))
            n = pace_j * factor * r
            a = jnp.exp2(n)
            c = 2.0 * LN2
            series = n * (n * (n * (-(c**3) / 6) - c * c / 2) - c)
            gain = jnp.where(n > -SMALL, series, 1.0 - a * a)
            b = gain * lax.rsqrt(jnp.maximum(gain, TINY)) * i * values[part]
            if h is None:
                h, total_a = b, a
            else:
                h = a * h + b
                total_a = total_a * a
            place = slice(SUB * (first_step + j), SUB * (first_step + j + 1))
            hloc[slot, place] = h
            acum[slot, place] = total_a

    def main_slot(slot):
        scan(convs[slot], slot, EDGE)

    def edge_slot(slot):
        scan(conv_edge(slot), slot, 0)
        edge_end = slice(SUB * (EDGE - 1), SUB * EDGE)
        chunk_end = slice(SUB * (steps - 1), SUB * steps)
        h = hloc[slot, chunk_end] + acum[slot, chunk_end] * hloc[slot, edge_end]
        totals(slot, h, acum[slot, chunk_end] * acum[slot, edge_end])

    def totals(slot, h, total_a):
        for shift in (1, 2, 4):
            inside = sub >= shift
            earlier_a = jnp.where(inside, pltpu.roll(total_a, shift, 0), 1.0)
            earlier_h = jnp.where(inside, pltpu.roll(h, shift, 0), 0.0)
            h = total_a * earlier_h + h
            total_a = total_a * earlier_a
        ex_h[slot] = jnp.where(sub >= 1, pltpu.roll(h, 1, 0), 0.0)
        ex_a[slot] = jnp.where(sub >= 1, pltpu.roll(total_a, 1, 0), 1.0)
        log_a = jnp.log2(jnp.maximum(total_a, TINY))
        for t in range(tiles):
            lanes = slice(LANES * t, LANES * (t + 1))
            stage[pl.ds(slot * tiles + t, 1), :] = log_a[SUB - 1 :, lanes]
            stage[pl.ds(lines + slot * tiles + t, 1), :] = h[SUB - 1 :, lanes]

    with scope("meet_early"):
        meet_early()
    with scope("loads"):
        for load in loads:
            load.wait()
    last[...] = x[count - SUB :, :].astype(jnp.float32)[SUB - CONV :].astype(jnp.bfloat16)
    with scope("meet_maps"):
        meet_maps()
    with scope("maps_a"):
        for load in map_loads[:FIRST]:
            load.wait()
        for own in range(min(FIRST, hl)):
            for copy in w_copies[own::hl]:
                copy.start()

    def send_halo():
        if root > 0:

            @pl.when(me < root)
            def _():
                halo_copy.start()

    with scope("meet_halo"):
        meet_halo()
    send_halo()

    spread = jnp.broadcast_to(pace_row[...], (LANES, count)).T
    pace_mat[...] = spread
    for j in range(steps):
        pace_perm[j] = pace_mat[pl.ds(j, SUB, stride=steps), :]

    with scope("conv_own"):
        for slot in range(hl):
            conv_main(slot)
    with scope("maps_b"):
        for load in map_loads[FIRST:]:
            load.wait()
        for own in range(FIRST, hl):
            for copy in w_copies[own::hl]:
                copy.start()
    with scope("own"):
        for slot in range(hl):
            main_slot(slot)
        for slot in range(hl, heads):
            conv_main(slot)
    for slot in range(hl, heads):
        with scope("map%d" % slot):
            w_copies[slot - hl].wait_recv()
        with scope("main%d" % slot):
            main_slot(slot)
    with scope("take_halo"):

        @pl.when(me > 0)
        def _():
            halo_copy.wait_recv()

    with scope("edges"):
        for slot in range(heads):
            edge_slot(slot)
        send_buf[...] = stage[...].astype(jnp.bfloat16)
    with scope("all_in"):

        @pl.when(me < root)
        def _():
            pl.semaphore_wait(known, 1)

    planes = -(-nsp // ROW)

    @pl.when(me == 0)
    def _():
        for rest in reversed(range(ROW)):
            for plane in reversed(range(planes)):
                if 0 < ROW * plane + rest < nsp:
                    carry_copy(0, ROW * plane + rest, lines).start()

    @pl.when(me > 0)
    def _():
        at = lax.rem(me, ROW)
        for rest in (ROW - 1 - at, at + 1 - 2 * lax.rem(at, 2), lax.rem(at + 2, ROW), at):
            for plane in reversed(range(planes)):
                dst = ROW * plane + rest

                @pl.when(jnp.logical_and(me < dst, dst < nsp))
                def _(dst=dst):
                    carry_copy(me, dst).start()

    with scope("lay"):

        @pl.loop(0, heads)
        def _(slot):
            edge_end = slice(SUB * (EDGE - 1), SUB * EDGE)
            first_h, first_a = ex_h[slot], ex_a[slot]
            later_h = hloc[slot, edge_end] + acum[slot, edge_end] * first_h
            later_a = acum[slot, edge_end] * first_a
            for j in range(steps):
                place = slice(SUB * j, SUB * (j + 1))
                h = hloc[slot, place] + acum[slot, place] * (first_h if j < EDGE else later_h)
                total_a = acum[slot, place] * (first_a if j < EDGE else later_a)
                for t in range(tiles):
                    lanes = slice(LANES * t, LANES * (t + 1))
                    lay_h[t, place] = h[:, lanes]
                    lay_a[t, place] = total_a[:, lanes]
            for t in range(tiles):
                line = lax.rem(d * hl + slot, heads) * tiles + t
                for c in range(SUB):
                    for k in range(0, steps, SUB):
                        place = slice(steps * c + k, steps * c + k + SUB)
                        part_h[line, place] = lay_h[t, pl.ds(SUB * k + c, SUB, stride=SUB), :]
                        part_a[line, place] = lay_a[t, pl.ds(SUB * k + c, SUB, stride=SUB), :]

    with scope("carry"):
        for many in range(1, nsp):

            @pl.when(me == many)
            def _(many=many):
                carries((2 * many - 1) * lines).wait_recv()

    with scope("finish"):
        start = jnp.zeros(carry.shape, jnp.float32)
        for src in range(root):
            got = recv_buf[2 * lines * src : 2 * lines * (src + 1)].astype(jnp.float32)
            start = jnp.exp2(got[:lines]) * start + got[lines:]
        for slot in range(heads):
            line = pl.multiple_of(lax.rem(d * hl + slot, heads) * tiles, tiles)
            carry[pl.ds(line, tiles), :] = start[slot * tiles : (slot + 1) * tiles]

    with scope("tail"):
        for copy in w_copies:
            copy.wait_send()

        if root > 0:

            @pl.when(me < root)
            def _():
                halo_copy.wait_send()

        for many in range(1, nsp):

            @pl.when(root - me == many)
            def _(many=many):
                carries((2 if many < root else 1) * many * lines).wait_send()


def finish(part_h, part_a, carry, out_hbm, out, sem):
    lines = carry.shape[0]
    count = out.shape[0]
    for low in range(0, count, 2 * SUB):
        rows = slice(low, low + 2 * SUB)
        for line in range(lines):
            state = part_h[line, rows] + part_a[line, rows] * carry[line : line + 1, :]
            out[rows, LANES * line : LANES * (line + 1)] = state.astype(jnp.bfloat16)
        pltpu.make_async_copy(out.at[rows], out_hbm.at[0, rows], sem).start()
    pltpu.make_async_copy(out, out_hbm.at[0], sem).wait()


def body(inputs, conv_weight, gate_weight, rate_param, pace):
    nsp = lax.axis_size("sp")
    ndp = lax.axis_size("dp")
    _, count, width = inputs.shape
    block = gate_weight.shape[-1]
    heads = width // block
    hl = heads // ndp
    lines = width // LANES
    f32, bf16 = jnp.float32, jnp.bfloat16
    hbm = pl.BlockSpec(memory_space=pltpu.HBM)
    dma = pltpu.SemaphoreType.DMA
    part_h, part_a, carry = pl.pallas_call(
        functools.partial(kernel, nsp, ndp, heads, block),
        out_shape=(
            pltpu.VMEM((lines, count, LANES), f32),
            pltpu.VMEM((lines, count, LANES), f32),
            pltpu.VMEM((lines, LANES), f32),
        ),
        in_specs=[hbm] * 5,
        out_specs=[pl.BlockSpec(memory_space=pltpu.VMEM)] * 3,
        scratch_shapes=[
            pltpu.VMEM((count, width), bf16),
            pltpu.VMEM(conv_weight.shape, bf16),
            pltpu.VMEM((2, heads, block, block), bf16),
            pltpu.VMEM((1, width), f32),
            pltpu.VMEM((1, count), f32),
            pltpu.VMEM((count, LANES), f32),
            pltpu.VMEM((count // SUB, SUB, LANES), f32),
            pltpu.VMEM((CONV, width), bf16),
            pltpu.VMEM((CONV, width), bf16),
            pltpu.VMEM((heads, 2 * EDGE * SUB, block), f32),
            pltpu.VMEM((heads, count - EDGE * SUB, block), f32),
            pltpu.VMEM((heads, count, block), f32),
            pltpu.VMEM((heads, count, block), f32),
            pltpu.VMEM((heads, SUB, block), f32),
            pltpu.VMEM((heads, SUB, block), f32),
            pltpu.VMEM((block // LANES, count, LANES), f32),
            pltpu.VMEM((block // LANES, count, LANES), f32),
            pltpu.VMEM((2 * lines, LANES), f32),
            pltpu.VMEM((2 * lines, LANES), bf16),
            pltpu.VMEM((2 * lines * nsp, LANES), bf16),
            pltpu.SemaphoreType.REGULAR,
            pltpu.SemaphoreType.REGULAR,
            dma,
            dma((2,)),
            dma,
            dma((heads - hl,)),
            dma,
            dma,
            dma,
            dma,
        ],
        compiler_params=pltpu.CompilerParams(collective_id=0, has_side_effects=True),
    )(inputs, conv_weight, gate_weight, rate_param.reshape(1, width), pace)
    return pl.pallas_call(
        finish,
        out_shape=jax.ShapeDtypeStruct(inputs.shape, bf16),
        in_specs=[pl.BlockSpec(memory_space=pltpu.VMEM)] * 3,
        out_specs=hbm,
        scratch_shapes=[pltpu.VMEM((count, width), bf16), dma],
        compiler_params=pltpu.CompilerParams(vmem_limit_bytes=8 * 2**20),
    )(part_h, part_a, carry)


def solution(mesh):
    return jax.shard_map(
        body,
        mesh=mesh,
        in_specs=(P("dp", "sp", None), P(), P(None, "dp", None, None), P(), P("dp", None)),
        out_specs=P("dp", "sp", None),
        check_vma=False,
    )
```

```python
import functools
import math

import jax
import jax.numpy as jnp
from jax import lax
from jax.experimental import pallas as pl
from jax.experimental.pallas import tpu as pltpu
from jax.sharding import PartitionSpec as P

CONV = 4
EDGE = CONV - 1
gate_power = 8.0
SUB = 8
LANES = 128
TINY = 1.2e-38
LN2 = math.log(2.0)
LOG2E = 1.0 / LN2
SMALL = 0.015
ROW = 4
FIRST = 2
MESH = pl.DeviceIdType.MESH


def softplus_neg(rate):
    e = jnp.exp(-jnp.abs(rate))
    series = e * (1.0 + e * (-0.5 + e * (1.0 / 3.0 + e * (-0.25 + e * 0.2))))
    return jnp.maximum(-rate, 0.0) + jnp.where(e < 0.03, series, jnp.log(1.0 + e))


def kernel(
    nsp, ndp, heads, block,
    x_hbm, cw_hbm, w_hbm, rate_hbm, pace_hbm, part_h, part_a, carry,
    x, cw, w, rate, pace_row, pace_mat, pace_perm, last, halo,
    convs, conv0, hloc, acum, all_h, all_a, edge_h, edge_a, ex_h, ex_a, lay_h, lay_a, stage, send_buf, recv_buf,
    known, met, load_sem, map_sem, w_send, w_recv, halo_send, halo_recv, c_send, c_recv,
):
    me = lax.axis_index("sp")
    d = lax.axis_index("dp")
    count, width = x.shape
    steps = count // SUB
    hl = heads // ndp
    tiles = block // LANES
    lines = heads * tiles
    root = nsp - 1
    relay = nsp // 2 + 1 if nsp >= 2 * ROW else 0
    reach = nsp // 2 + ROW - 1
    near = 2
    scope = jax.named_scope

    first = pl.multiple_of(me * count, count)
    loads = [
        pltpu.make_async_copy(x_hbm.at[0], x, load_sem),
        pltpu.make_async_copy(cw_hbm, cw, load_sem),
        pltpu.make_async_copy(rate_hbm, rate, load_sem),
        pltpu.make_async_copy(pace_hbm.at[:, pl.ds(first, count)], pace_row, load_sem),
    ]
    map_loads = [
        pltpu.make_async_copy(w_hbm.at[:, own], w.at[:, own], map_sem.at[int(own >= FIRST)])
        for own in range(hl)
    ]
    for load in loads + map_loads:
        load.start()

    recv_buf[...] = jnp.zeros_like(recv_buf)

    barrier = pltpu.get_barrier_semaphore()

    def greet(there):
        pl.semaphore_signal(barrier, inc=1, device_id={"sp": there}, device_id_type=MESH)

    @pl.loop(d + 1, ndp)
    def _(o):
        pl.semaphore_signal(barrier, inc=1, device_id={"dp": o}, device_id_type=MESH)

    if root > 0:

        @pl.when(me > 0)
        def _():
            greet(me - 1)

    if root > 1:

        @pl.when(me < root - 1)
        def _():
            greet(root)

        @pl.when(me == root - 1)
        def _():
            greet(root)

    if relay:

        @pl.when(jnp.logical_and(d == 0, (me <= reach) & (me != relay) & (me != relay + 1)))
        def _():
            greet(relay)

    @pl.when(me == 0)
    def _():
        halo[...] = jnp.zeros_like(halo)

    def meet():
        expect = jnp.where(me == root, root if root > 1 else 0, min(root, 1))
        if relay:
            expect = jnp.where(jnp.logical_and(d == 0, me == relay), reach, expect)
        pl.semaphore_wait(barrier, d + expect)

    def meet_early():
        if root > 0:

            @pl.when(me == root)
            def _():
                meet()
                for there in range(root):
                    pl.semaphore_signal(known.at[0], inc=1, device_id={"sp": there}, device_id_type=MESH)

    def meet_maps():
        @pl.when(jnp.logical_and(me < max(root, 1), d > 0))
        def _():
            meet()

        @pl.loop(0, d)
        def _(o):
            pl.semaphore_signal(met, inc=1, device_id={"dp": o}, device_id_type=MESH)

        @pl.when(d < ndp - 1)
        def _():
            pl.semaphore_wait(met, ndp - 1 - d)

    def meet_halo():
        @pl.when(jnp.logical_and(me < root, d == 0))
        def _():
            meet()

            if relay:

                @pl.when(me == relay)
                def _():
                    for there in range(near):
                        pl.semaphore_signal(known.at[1], inc=1, device_id={"sp": there}, device_id_type=MESH)

    w_copies = []
    for slot in range(hl, heads):
        o, own = slot // hl, slot % hl
        w_copies.append(pltpu.make_async_remote_copy(
            src_ref=w.at[:, own],
            dst_ref=w.at[:, slot],
            send_sem=w_send,
            recv_sem=w_recv.at[slot - hl],
            device_id={"dp": lax.rem(d - o + ndp, ndp)},
            device_id_type=MESH,
        ))
    halo_copy = pltpu.make_async_remote_copy(
        src_ref=last,
        dst_ref=halo,
        send_sem=halo_send,
        recv_sem=halo_recv,
        device_id={"sp": lax.rem(me + 1, nsp)},
        device_id_type=MESH,
    )

    def carry_copy(src, dst, low=0):
        return pltpu.make_async_remote_copy(
            src_ref=send_buf.at[pl.ds(low, 2 * lines - low)],
            dst_ref=recv_buf.at[pl.ds(2 * lines * src + low, 2 * lines - low)],
            send_sem=c_send,
            recv_sem=c_recv,
            device_id={"sp": dst},
            device_id_type=MESH,
        )

    def carries(rows):
        block = recv_buf.at[pl.ds(0, rows)]
        return pltpu.make_async_remote_copy(
            src_ref=block,
            dst_ref=block,
            send_sem=c_send,
            recv_sem=c_recv,
            device_id={"sp": root - me},
            device_id_type=MESH,
        )

    row = lax.broadcasted_iota(jnp.int32, (count, count), 0)
    col = lax.broadcasted_iota(jnp.int32, (count, count), 1)
    gather = jnp.where(col == (row % SUB) * steps + row // SUB, 1.0, 0.0).astype(jnp.bfloat16)
    sub = lax.broadcasted_iota(jnp.int32, (SUB, block), 0)

    def columns(slot):
        return pl.ds(pl.multiple_of(lax.rem(d * hl + slot, heads) * block, block), block)

    def convolve(rows, here):
        taps = cw[:, here].astype(jnp.float32)
        taps = [jnp.broadcast_to(taps[k : k + 1], (SUB, block)) for k in range(CONV)]
        out = []
        for j in range(len(rows) - EDGE):
            total = taps[0] * rows[j]
            for k in range(1, CONV):
                total = total + taps[k] * rows[j + k]
            out.append(total)
        return jnp.concatenate(out, axis=0)

    def conv_main(slot):
        here = columns(slot)
        xp = jnp.dot(gather, x[:, here], preferred_element_type=jnp.float32)
        rows = [xp[SUB * j : SUB * (j + 1)] for j in range(steps)]
        rows = [pltpu.roll(rows[steps - EDGE + j], 1, 0) for j in range(EDGE)] + rows
        convs[slot] = convolve(rows, here)

    def gates(conv, slot, pace_of):
        conv = conv.astype(jnp.bfloat16)
        pre_r = jnp.dot(conv, w[0, slot], preferred_element_type=jnp.float32)
        pre_i = jnp.dot(conv, w[1, slot], preferred_element_type=jnp.float32)
        values = conv.astype(jnp.float32)
        factor = softplus_neg(rate[:, columns(slot)]) * (-gate_power / LN2)
        factor = jnp.broadcast_to(factor, (SUB, block))
        for j in range(conv.shape[0] // SUB):
            part = slice(SUB * j, SUB * (j + 1))
            pace_j = jnp.concatenate([pace_of(j)] * tiles, axis=1)
            r = 1.0 / (1.0 + jnp.exp2(pre_r[part] * -LOG2E))
            i = 1.0 / (1.0 + jnp.exp2(pre_i[part] * -LOG2E))
            n = pace_j * factor * r
            a = jnp.exp2(n)
            c = 2.0 * LN2
            series = n * (n * (n * (-(c**3) / 6) - c * c / 2) - c)
            gain = jnp.where(n > -SMALL, series, 1.0 - a * a)
            b = gain * lax.rsqrt(jnp.maximum(gain, TINY)) * i * values[part]
            yield a, b

    def prefix(h, total_a, shifts):
        for shift in shifts:
            inside = sub >= shift
            earlier_a = jnp.where(inside, pltpu.roll(total_a, shift, 0), 1.0)
            earlier_h = jnp.where(inside, pltpu.roll(h, shift, 0), 0.0)
            h = total_a * earlier_h + h
            total_a = total_a * earlier_a
        return h, total_a

    def main_slot(slot):
        for j, (a, b) in enumerate(gates(convs[slot], slot, lambda j: pace_perm[j])):
            if j == 0:
                h, total_a = b, a
            elif j == EDGE:
                h = jnp.where(sub == 0, b, a * h + b)
                total_a = jnp.where(sub == 0, a, total_a * a)
            else:
                h = a * h + b
                total_a = total_a * a
            place = slice(SUB * j, SUB * (j + 1))
            hloc[slot, place] = h
            acum[slot, place] = total_a
        h, total_a = prefix(h, total_a, (1, 2, 4))
        all_h[slot] = h
        all_a[slot] = total_a

    def conv_edge():
        own = pltpu.roll(x[:SUB, :].astype(jnp.float32), EDGE, 0)
        before = jnp.concatenate([halo[...].astype(jnp.float32)] * (SUB // CONV), axis=0)
        wide = lax.broadcasted_iota(jnp.int32, own.shape, 0)
        rows = jnp.where(wide < EDGE, before, own)
        taps = cw[...].astype(jnp.float32)
        total = taps[0:1] * rows
        for k in range(1, CONV):
            total = total + taps[k : k + 1] * pltpu.roll(rows, SUB - k, 0)
        conv0[...] = total

    def edge_slot(slot):
        (a, b), = gates(conv0[:, columns(slot)], slot, lambda j: pace_mat[:SUB, :])
        h, total_a = prefix(b, a, (1, 2))
        edge_h[slot] = h
        edge_a[slot] = total_a
        first_h = jnp.broadcast_to(h[EDGE - 1 : EDGE], (SUB, block))
        first_a = jnp.broadcast_to(total_a[EDGE - 1 : EDGE], (SUB, block))
        h, total_a = all_h[slot], all_a[slot]
        before_h = jnp.where(sub >= 1, pltpu.roll(h, 1, 0), 0.0)
        before_a = jnp.where(sub >= 1, pltpu.roll(total_a, 1, 0), 1.0)
        ex_h[slot] = before_h + before_a * first_h
        ex_a[slot] = before_a * first_a
        h = h + total_a * first_h
        log_a = jnp.log2(jnp.maximum(total_a * first_a, TINY))
        for t in range(tiles):
            lanes = slice(LANES * t, LANES * (t + 1))
            stage[pl.ds(slot * tiles + t, 1), :] = log_a[SUB - 1 :, lanes]
            stage[pl.ds(lines + slot * tiles + t, 1), :] = h[SUB - 1 :, lanes]

    with scope("meet_early"):
        meet_early()
    with scope("loads"):
        for load in loads:
            load.wait()
    last[...] = pltpu.roll(x[count - SUB :, :].astype(jnp.float32), EDGE, 0)[:CONV].astype(jnp.bfloat16)
    with scope("meet_maps"):
        meet_maps()
    with scope("maps_a"):
        for load in map_loads[:FIRST]:
            load.wait()
        for own in range(min(FIRST, hl)):
            for copy in w_copies[own::hl]:
                copy.start()

    def send_halo():
        if root > 0:

            @pl.when(me < root)
            def _():
                halo_copy.start()

    with scope("meet_halo"):
        meet_halo()
    send_halo()

    spread = jnp.broadcast_to(pace_row[...], (LANES, count)).T
    pace_mat[...] = spread
    for j in range(steps):
        pace_perm[j] = pace_mat[pl.ds(j, SUB, stride=steps), :]

    with scope("conv_own"):
        for slot in range(hl):
            conv_main(slot)
    with scope("maps_b"):
        for load in map_loads[FIRST:]:
            load.wait()
        for own in range(FIRST, hl):
            for copy in w_copies[own::hl]:
                copy.start()
    turns = [list(range(hl)), list(range(hl, heads))[:2]] + [[slot] for slot in range(hl + 2, heads)]
    turns = [turn for turn in turns if turn]
    for turn, after in zip(turns, turns[1:] + [[]]):
        if not after:
            with scope("take_halo"):

                @pl.when(me > 0)
                def _():
                    halo_copy.wait_recv()

        with scope("map%d" % turn[0]):
            for slot in turn:
                if slot >= hl:
                    w_copies[slot - hl].wait_recv()
        with scope("main%d" % turn[0]):
            for slot in turn:
                main_slot(slot)
            for slot in after:
                conv_main(slot)
            if not after:
                conv_edge()
                for slot in range(heads):
                    edge_slot(slot)
                send_buf[...] = stage[...].astype(jnp.bfloat16)
    planes = -(-nsp // ROW)
    split = reach // ROW + 1 if relay else 0
    early = jnp.logical_and(me < near, d == 0) if relay else me < 0

    def all_in():
        if root > 0:

            @pl.when(me < root)
            def _():
                pl.semaphore_wait(known.at[0], 1)

    def send_first(low, high):
        for rest in reversed(range(ROW)):
            for plane in reversed(range(low, high)):
                if 0 < ROW * plane + rest < nsp:
                    carry_copy(0, ROW * plane + rest, lines).start()

    def send_rest(low, high):
        at = lax.rem(me, ROW)
        for rest in (ROW - 1 - at, at + 1 - 2 * lax.rem(at, 2), lax.rem(at + 2, ROW), at):
            for plane in reversed(range(low, high)):
                dst = ROW * plane + rest

                @pl.when(jnp.logical_and(me < dst, dst < nsp))
                def _(dst=dst):
                    carry_copy(me, dst).start()

    def send(low, high):
        @pl.when(me == 0)
        def _():
            send_first(low, high)

        @pl.when(me > 0)
        def _():
            send_rest(low, high)

    if relay:

        @pl.when(early)
        def _():
            pl.semaphore_wait(known.at[1], 1)
            send(0, split)

    with scope("all_in"):
        all_in()

    if relay:

        @pl.when(early)
        def _():
            send(split, planes)

    @pl.when(jnp.logical_not(early))
    def _():
        send(0, planes)

    with scope("lay"):

        @pl.loop(0, heads)
        def _(slot):
            before_h, before_a = ex_h[slot], ex_a[slot]
            for j in range(steps):
                place = slice(SUB * j, SUB * (j + 1))
                h = hloc[slot, place] + acum[slot, place] * before_h
                total_a = acum[slot, place] * before_a
                if j < EDGE:
                    h = jnp.where(sub == 0, edge_h[slot, j : j + 1], h)
                    total_a = jnp.where(sub == 0, edge_a[slot, j : j + 1], total_a)
                for t in range(tiles):
                    lanes = slice(LANES * t, LANES * (t + 1))
                    lay_h[t, place] = h[:, lanes]
                    lay_a[t, place] = total_a[:, lanes]
            for t in range(tiles):
                line = lax.rem(d * hl + slot, heads) * tiles + t
                for c in range(SUB):
                    for k in range(0, steps, SUB):
                        place = slice(steps * c + k, steps * c + k + SUB)
                        part_h[line, place] = lay_h[t, pl.ds(SUB * k + c, SUB, stride=SUB), :]
                        part_a[line, place] = lay_a[t, pl.ds(SUB * k + c, SUB, stride=SUB), :]

    with scope("carry"):
        for many in range(1, nsp):

            @pl.when(me == many)
            def _(many=many):
                carries((2 * many - 1) * lines).wait_recv()

    with scope("finish"):
        start = jnp.zeros(carry.shape, jnp.float32)
        for src in range(root):
            got = recv_buf[2 * lines * src : 2 * lines * (src + 1)].astype(jnp.float32)
            start = jnp.exp2(got[:lines]) * start + got[lines:]
        for slot in range(heads):
            line = pl.multiple_of(lax.rem(d * hl + slot, heads) * tiles, tiles)
            carry[pl.ds(line, tiles), :] = start[slot * tiles : (slot + 1) * tiles]

    with scope("tail"):
        for copy in w_copies:
            copy.wait_send()

        if root > 0:

            @pl.when(me < root)
            def _():
                halo_copy.wait_send()

        for many in range(1, nsp):

            @pl.when(root - me == many)
            def _(many=many):
                carries((2 if many < root else 1) * many * lines).wait_send()


def finish(part_h, part_a, carry, out_hbm, out, sem):
    lines = carry.shape[0]
    count = out.shape[0]
    for low in range(0, count, 2 * SUB):
        rows = slice(low, low + 2 * SUB)
        for line in range(lines):
            state = part_h[line, rows] + part_a[line, rows] * carry[line : line + 1, :]
            out[rows, LANES * line : LANES * (line + 1)] = state.astype(jnp.bfloat16)
        pltpu.make_async_copy(out.at[rows], out_hbm.at[0, rows], sem).start()
    pltpu.make_async_copy(out, out_hbm.at[0], sem).wait()


def body(inputs, conv_weight, gate_weight, rate_param, pace):
    nsp = lax.axis_size("sp")
    ndp = lax.axis_size("dp")
    _, count, width = inputs.shape
    block = gate_weight.shape[-1]
    heads = width // block
    hl = heads // ndp
    lines = width // LANES
    f32, bf16 = jnp.float32, jnp.bfloat16
    hbm = pl.BlockSpec(memory_space=pltpu.HBM)
    dma = pltpu.SemaphoreType.DMA
    part_h, part_a, carry = pl.pallas_call(
        functools.partial(kernel, nsp, ndp, heads, block),
        out_shape=(
            pltpu.VMEM((lines, count, LANES), f32),
            pltpu.VMEM((lines, count, LANES), f32),
            pltpu.VMEM((lines, LANES), f32),
        ),
        in_specs=[hbm] * 5,
        out_specs=[pl.BlockSpec(memory_space=pltpu.VMEM)] * 3,
        scratch_shapes=[
            pltpu.VMEM((count, width), bf16),
            pltpu.VMEM(conv_weight.shape, bf16),
            pltpu.VMEM((2, heads, block, block), bf16),
            pltpu.VMEM((1, width), f32),
            pltpu.VMEM((1, count), f32),
            pltpu.VMEM((count, LANES), f32),
            pltpu.VMEM((count // SUB, SUB, LANES), f32),
            pltpu.VMEM((CONV, width), bf16),
            pltpu.VMEM((CONV, width), bf16),
            pltpu.VMEM((heads, count, block), f32),
            pltpu.VMEM((SUB, width), f32),
            pltpu.VMEM((heads, count, block), f32),
            pltpu.VMEM((heads, count, block), f32),
            pltpu.VMEM((heads, SUB, block), f32),
            pltpu.VMEM((heads, SUB, block), f32),
            pltpu.VMEM((heads, SUB, block), f32),
            pltpu.VMEM((heads, SUB, block), f32),
            pltpu.VMEM((heads, SUB, block), f32),
            pltpu.VMEM((heads, SUB, block), f32),
            pltpu.VMEM((block // LANES, count, LANES), f32),
            pltpu.VMEM((block // LANES, count, LANES), f32),
            pltpu.VMEM((2 * lines, LANES), f32),
            pltpu.VMEM((2 * lines, LANES), bf16),
            pltpu.VMEM((2 * lines * nsp, LANES), bf16),
            pltpu.SemaphoreType.REGULAR((2,)),
            pltpu.SemaphoreType.REGULAR,
            dma,
            dma((2,)),
            dma,
            dma((heads - hl,)),
            dma,
            dma,
            dma,
            dma,
        ],
        compiler_params=pltpu.CompilerParams(collective_id=0, has_side_effects=True),
    )(inputs, conv_weight, gate_weight, rate_param.reshape(1, width), pace)
    return pl.pallas_call(
        finish,
        out_shape=jax.ShapeDtypeStruct(inputs.shape, bf16),
        in_specs=[pl.BlockSpec(memory_space=pltpu.VMEM)] * 3,
        out_specs=hbm,
        scratch_shapes=[pltpu.VMEM((count, width), bf16), dma],
        compiler_params=pltpu.CompilerParams(vmem_limit_bytes=8 * 2**20),
    )(part_h, part_a, carry)


def solution(mesh):
    return jax.shard_map(
        body,
        mesh=mesh,
        in_specs=(P("dp", "sp", None), P(), P(None, "dp", None, None), P(), P("dp", None)),
        out_specs=P("dp", "sp", None),
        check_vma=False,
    )
```

```python
import functools
import math

import jax
import jax.numpy as jnp
from jax import lax
from jax.experimental import pallas as pl
from jax.experimental.pallas import tpu as pltpu
from jax.sharding import PartitionSpec as P

CONV = 4
EDGE = CONV - 1
gate_power = 8.0
SUB = 8
LANES = 128
TINY = 1.2e-38
LN2 = math.log(2.0)
LOG2E = 1.0 / LN2
SMALL = 0.015
ROW = 4
FIRST = 2
MESH = pl.DeviceIdType.MESH


def softplus_neg(rate):
    e = jnp.exp(-jnp.abs(rate))
    series = e * (1.0 + e * (-0.5 + e * (1.0 / 3.0 + e * (-0.25 + e * 0.2))))
    return jnp.maximum(-rate, 0.0) + jnp.where(e < 0.03, series, jnp.log(1.0 + e))


def kernel(
    nsp, ndp, heads, block,
    x_hbm, cw_hbm, w_hbm, rate_hbm, pace_hbm, part_h, part_a, carry,
    x, cw, w, rate, pace_row, pace_mat, pace_perm, last, halo,
    convs, conv0, hloc, acum, all_h, all_a, edge_h, edge_a, ex_h, ex_a, lay_h, lay_a, stage, send_buf, recv_buf,
    known, met, load_sem, map_sem, w_send, w_recv, halo_send, halo_recv, c_send, c_recv,
):
    me = lax.axis_index("sp")
    d = lax.axis_index("dp")
    count, width = x.shape
    steps = count // SUB
    hl = heads // ndp
    tiles = block // LANES
    lines = heads * tiles
    root = nsp - 1
    relay = nsp // 2 + 1 if nsp >= 2 * ROW else 0
    reach = nsp // 2 + ROW - 1
    near = 2
    scope = jax.named_scope

    first = pl.multiple_of(me * count, count)
    loads = [
        pltpu.make_async_copy(x_hbm.at[0], x, load_sem),
        pltpu.make_async_copy(cw_hbm, cw, load_sem),
        pltpu.make_async_copy(rate_hbm, rate, load_sem),
        pltpu.make_async_copy(pace_hbm.at[:, pl.ds(first, count)], pace_row, load_sem),
    ]
    map_loads = [
        pltpu.make_async_copy(w_hbm.at[:, own], w.at[:, own], map_sem.at[int(own >= FIRST)])
        for own in range(hl)
    ]
    for load in loads + map_loads:
        load.start()

    recv_buf[...] = jnp.zeros_like(recv_buf)

    barrier = pltpu.get_barrier_semaphore()

    def greet(there):
        pl.semaphore_signal(barrier, inc=1, device_id={"sp": there}, device_id_type=MESH)

    @pl.loop(d + 1, ndp)
    def _(o):
        pl.semaphore_signal(barrier, inc=1, device_id={"dp": o}, device_id_type=MESH)

    if root > 0:

        @pl.when(me > 0)
        def _():
            greet(me - 1)

    if root > 1:

        @pl.when(me < root - 1)
        def _():
            greet(root)

        @pl.when(me == root - 1)
        def _():
            greet(root)

    if relay:

        @pl.when(jnp.logical_and(d == 0, (me <= reach) & (me != relay) & (me != relay + 1)))
        def _():
            greet(relay)

    @pl.when(me == 0)
    def _():
        halo[...] = jnp.zeros_like(halo)

    def meet():
        expect = jnp.where(me == root, root if root > 1 else 0, min(root, 1))
        if relay:
            expect = jnp.where(jnp.logical_and(d == 0, me == relay), reach, expect)
        pl.semaphore_wait(barrier, d + expect)

    def meet_early():
        if root > 0:

            @pl.when(me == root)
            def _():
                meet()
                for there in range(root):
                    pl.semaphore_signal(known.at[0], inc=1, device_id={"sp": there}, device_id_type=MESH)

    def meet_maps():
        @pl.when(jnp.logical_and(me < max(root, 1), d > 0))
        def _():
            meet()

        @pl.loop(0, d)
        def _(o):
            pl.semaphore_signal(met, inc=1, device_id={"dp": o}, device_id_type=MESH)

        @pl.when(d < ndp - 1)
        def _():
            pl.semaphore_wait(met, ndp - 1 - d)

    def meet_halo():
        @pl.when(jnp.logical_and(me < root, d == 0))
        def _():
            meet()

            if relay:

                @pl.when(me == relay)
                def _():
                    for there in range(near):
                        pl.semaphore_signal(known.at[1], inc=1, device_id={"sp": there}, device_id_type=MESH)

    w_copies = []
    for slot in range(hl, heads):
        o, own = slot // hl, slot % hl
        w_copies.append(pltpu.make_async_remote_copy(
            src_ref=w.at[:, own],
            dst_ref=w.at[:, slot],
            send_sem=w_send,
            recv_sem=w_recv.at[slot - hl],
            device_id={"dp": lax.rem(d - o + ndp, ndp)},
            device_id_type=MESH,
        ))
    halo_copy = pltpu.make_async_remote_copy(
        src_ref=last,
        dst_ref=halo,
        send_sem=halo_send,
        recv_sem=halo_recv,
        device_id={"sp": lax.rem(me + 1, nsp)},
        device_id_type=MESH,
    )

    def carry_copy(src, dst, low=0):
        return pltpu.make_async_remote_copy(
            src_ref=send_buf.at[pl.ds(low, 2 * lines - low)],
            dst_ref=recv_buf.at[pl.ds(2 * lines * src + low, 2 * lines - low)],
            send_sem=c_send,
            recv_sem=c_recv,
            device_id={"sp": dst},
            device_id_type=MESH,
        )

    def carries(rows):
        block = recv_buf.at[pl.ds(0, rows)]
        return pltpu.make_async_remote_copy(
            src_ref=block,
            dst_ref=block,
            send_sem=c_send,
            recv_sem=c_recv,
            device_id={"sp": root - me},
            device_id_type=MESH,
        )

    row = lax.broadcasted_iota(jnp.int32, (count, count), 0)
    col = lax.broadcasted_iota(jnp.int32, (count, count), 1)
    gather = jnp.where(col == (row % SUB) * steps + row // SUB, 1.0, 0.0).astype(jnp.bfloat16)
    sub = lax.broadcasted_iota(jnp.int32, (SUB, block), 0)

    def columns(slot):
        return pl.ds(pl.multiple_of(lax.rem(d * hl + slot, heads) * block, block), block)

    def convolve(rows, here):
        taps = cw[:, here].astype(jnp.float32)
        taps = [jnp.broadcast_to(taps[k : k + 1], (SUB, block)) for k in range(CONV)]
        out = []
        for j in range(len(rows) - EDGE):
            total = taps[0] * rows[j]
            for k in range(1, CONV):
                total = total + taps[k] * rows[j + k]
            out.append(total)
        return jnp.concatenate(out, axis=0)

    def conv_main(slot):
        here = columns(slot)
        xp = jnp.dot(gather, x[:, here], preferred_element_type=jnp.float32)
        rows = [xp[SUB * j : SUB * (j + 1)] for j in range(steps)]
        rows = [pltpu.roll(rows[steps - EDGE + j], 1, 0) for j in range(EDGE)] + rows
        convs[slot] = convolve(rows, here)

    def gates(conv, slot, pace_of):
        conv = conv.astype(jnp.bfloat16)
        pre_r = jnp.dot(conv, w[0, slot], preferred_element_type=jnp.float32)
        pre_i = jnp.dot(conv, w[1, slot], preferred_element_type=jnp.float32)
        values = conv.astype(jnp.float32)
        factor = softplus_neg(rate[:, columns(slot)]) * (-gate_power / LN2)
        factor = jnp.broadcast_to(factor, (SUB, block))
        for j in range(conv.shape[0] // SUB):
            part = slice(SUB * j, SUB * (j + 1))
            pace_j = jnp.concatenate([pace_of(j)] * tiles, axis=1)
            r = 1.0 / (1.0 + jnp.exp2(pre_r[part] * -LOG2E))
            i = 1.0 / (1.0 + jnp.exp2(pre_i[part] * -LOG2E))
            n = pace_j * factor * r
            a = jnp.exp2(n)
            c = 2.0 * LN2
            series = n * (n * (n * (-(c**3) / 6) - c * c / 2) - c)
            gain = jnp.where(n > -SMALL, series, 1.0 - a * a)
            b = gain * lax.rsqrt(jnp.maximum(gain, TINY)) * i * values[part]
            yield a, b

    def prefix(h, total_a, shifts):
        for shift in shifts:
            inside = sub >= shift
            earlier_a = jnp.where(inside, pltpu.roll(total_a, shift, 0), 1.0)
            earlier_h = jnp.where(inside, pltpu.roll(h, shift, 0), 0.0)
            h = total_a * earlier_h + h
            total_a = total_a * earlier_a
        return h, total_a

    def main_slot(slot):
        for j, (a, b) in enumerate(gates(convs[slot], slot, lambda j: pace_perm[j])):
            if j == 0:
                h, total_a = b, a
            elif j == EDGE:
                h = jnp.where(sub == 0, b, a * h + b)
                total_a = jnp.where(sub == 0, a, total_a * a)
            else:
                h = a * h + b
                total_a = total_a * a
            place = slice(SUB * j, SUB * (j + 1))
            hloc[slot, place] = h
            acum[slot, place] = total_a
        h, total_a = prefix(h, total_a, (1, 2, 4))
        all_h[slot] = h
        all_a[slot] = total_a

    def conv_edge():
        own = pltpu.roll(x[:SUB, :].astype(jnp.float32), EDGE, 0)
        before = jnp.concatenate([halo[...].astype(jnp.float32)] * (SUB // CONV), axis=0)
        wide = lax.broadcasted_iota(jnp.int32, own.shape, 0)
        rows = jnp.where(wide < EDGE, before, own)
        taps = cw[...].astype(jnp.float32)
        total = taps[0:1] * rows
        for k in range(1, CONV):
            total = total + taps[k : k + 1] * pltpu.roll(rows, SUB - k, 0)
        conv0[...] = total

    def edge_slot(slot):
        (a, b), = gates(conv0[:, columns(slot)], slot, lambda j: pace_mat[:SUB, :])
        h, total_a = prefix(b, a, (1, 2))
        edge_h[slot] = h
        edge_a[slot] = total_a
        first_h = jnp.broadcast_to(h[EDGE - 1 : EDGE], (SUB, block))
        first_a = jnp.broadcast_to(total_a[EDGE - 1 : EDGE], (SUB, block))
        h, total_a = all_h[slot], all_a[slot]
        before_h = jnp.where(sub >= 1, pltpu.roll(h, 1, 0), 0.0)
        before_a = jnp.where(sub >= 1, pltpu.roll(total_a, 1, 0), 1.0)
        ex_h[slot] = before_h + before_a * first_h
        ex_a[slot] = before_a * first_a
        h = h + total_a * first_h
        log_a = jnp.log2(jnp.maximum(total_a * first_a, TINY))
        for t in range(tiles):
            lanes = slice(LANES * t, LANES * (t + 1))
            stage[pl.ds(slot * tiles + t, 1), :] = log_a[SUB - 1 :, lanes]
            stage[pl.ds(lines + slot * tiles + t, 1), :] = h[SUB - 1 :, lanes]

    with scope("meet_early"):
        meet_early()
    with scope("loads"):
        for load in loads:
            load.wait()
    last[...] = pltpu.roll(x[count - SUB :, :].astype(jnp.float32), EDGE, 0)[:CONV].astype(jnp.bfloat16)
    with scope("meet_maps"):
        meet_maps()
    with scope("maps_a"):
        for load in map_loads[:FIRST]:
            load.wait()
        for own in range(min(FIRST, hl)):
            for copy in w_copies[own::hl]:
                copy.start()

    def send_halo():
        if root > 0:

            @pl.when(me < root)
            def _():
                halo_copy.start()

    @pl.when(d > 0)
    def _():
        send_halo()

    spread = jnp.broadcast_to(pace_row[...], (LANES, count)).T
    pace_mat[...] = spread
    for j in range(steps):
        pace_perm[j] = pace_mat[pl.ds(j, SUB, stride=steps), :]

    with scope("conv_a"):
        for slot in range(hl // 2):
            conv_main(slot)
    with scope("meet_halo"):
        meet_halo()

    @pl.when(d == 0)
    def _():
        send_halo()

    with scope("conv_b"):
        for slot in range(hl // 2, hl):
            conv_main(slot)
    with scope("maps_b"):
        for load in map_loads[FIRST:]:
            load.wait()
        for own in range(FIRST, hl):
            for copy in w_copies[own::hl]:
                copy.start()
    def wait_halo():
        with scope("take_halo"):

            @pl.when(me > 0)
            def _():
                halo_copy.wait_recv()

    def wait_maps(turn):
        with scope("map%d" % turn[0]):
            for slot in turn:
                if slot >= hl:
                    w_copies[slot - hl].wait_recv()

    def mains(turn, after=()):
        for slot in turn:
            main_slot(slot)
        for slot in after:
            conv_main(slot)

    def edges():
        conv_edge()
        for slot in range(heads):
            edge_slot(slot)
        send_buf[...] = stage[...].astype(jnp.bfloat16)

    turns = [list(range(hl)), list(range(hl, heads))[:2]] + [[slot] for slot in range(hl + 2, heads)]
    turns = [turn for turn in turns if turn]
    for turn, after in zip(turns, turns[1:]):
        wait_maps(turn)
        with scope("main%d" % turn[0]):
            mains(turn, after)

    @pl.when(d == 0)
    def _():
        wait_maps(turns[-1])
        with scope("last"):
            mains(turns[-1])
        wait_halo()
        with scope("edges"):
            edges()

    @pl.when(d > 0)
    def _():
        wait_halo()
        wait_maps(turns[-1])
        with scope("edges"):
            mains(turns[-1])
            edges()

    planes = -(-nsp // ROW)
    split = reach // ROW + 1 if relay else 0
    early = jnp.logical_and(me < near, d == 0) if relay else me < 0

    def all_in():
        if root > 0:

            @pl.when(me < root)
            def _():
                pl.semaphore_wait(known.at[0], 1)

    def send_first(low, high):
        for rest in reversed(range(ROW)):
            for plane in reversed(range(low, high)):
                if 0 < ROW * plane + rest < nsp:
                    carry_copy(0, ROW * plane + rest, lines).start()

    def send_rest(low, high):
        at = lax.rem(me, ROW)
        mid = 1 - lax.rem((at + 1) // 2, 2)
        for rest in (ROW - 1 - at, mid, ROW - 1 - mid, at):
            for plane in reversed(range(low, high)):
                dst = ROW * plane + rest

                @pl.when(jnp.logical_and(me < dst, dst < nsp))
                def _(dst=dst):
                    carry_copy(me, dst).start()

    def send(low, high):
        @pl.when(me == 0)
        def _():
            send_first(low, high)

        @pl.when(me > 0)
        def _():
            send_rest(low, high)

    if relay:

        @pl.when(early)
        def _():
            pl.semaphore_wait(known.at[1], 1)
            send(0, split)

    with scope("all_in"):
        all_in()

    if relay:

        @pl.when(early)
        def _():
            send(split, planes)

    @pl.when(jnp.logical_not(early))
    def _():
        send(0, planes)

    with scope("lay"):

        @pl.loop(0, heads)
        def _(slot):
            before_h, before_a = ex_h[slot], ex_a[slot]
            for j in range(steps):
                place = slice(SUB * j, SUB * (j + 1))
                h = hloc[slot, place] + acum[slot, place] * before_h
                total_a = acum[slot, place] * before_a
                if j < EDGE:
                    h = jnp.where(sub == 0, edge_h[slot, j : j + 1], h)
                    total_a = jnp.where(sub == 0, edge_a[slot, j : j + 1], total_a)
                for t in range(tiles):
                    lanes = slice(LANES * t, LANES * (t + 1))
                    lay_h[t, place] = h[:, lanes]
                    lay_a[t, place] = total_a[:, lanes]
            for t in range(tiles):
                line = lax.rem(d * hl + slot, heads) * tiles + t
                for c in range(SUB):
                    for k in range(0, steps, SUB):
                        place = slice(steps * c + k, steps * c + k + SUB)
                        part_h[line, place] = lay_h[t, pl.ds(SUB * k + c, SUB, stride=SUB), :]
                        part_a[line, place] = lay_a[t, pl.ds(SUB * k + c, SUB, stride=SUB), :]

    with scope("carry"):
        for many in range(1, nsp):

            @pl.when(me == many)
            def _(many=many):
                carries((2 * many - 1) * lines).wait_recv()

    with scope("finish"):
        start = jnp.zeros(carry.shape, jnp.float32)
        for src in range(root):
            got = recv_buf[2 * lines * src : 2 * lines * (src + 1)].astype(jnp.float32)
            start = jnp.exp2(got[:lines]) * start + got[lines:]
        for slot in range(heads):
            line = pl.multiple_of(lax.rem(d * hl + slot, heads) * tiles, tiles)
            carry[pl.ds(line, tiles), :] = start[slot * tiles : (slot + 1) * tiles]

    with scope("tail"):
        for copy in w_copies:
            copy.wait_send()

        if root > 0:

            @pl.when(me < root)
            def _():
                halo_copy.wait_send()

        for many in range(1, nsp):

            @pl.when(root - me == many)
            def _(many=many):
                carries((2 if many < root else 1) * many * lines).wait_send()


def finish(part_h, part_a, carry, out_hbm, out, sem):
    lines = carry.shape[0]
    count = out.shape[0]
    for low in range(0, count, 2 * SUB):
        rows = slice(low, low + 2 * SUB)
        for line in range(lines):
            state = part_h[line, rows] + part_a[line, rows] * carry[line : line + 1, :]
            out[rows, LANES * line : LANES * (line + 1)] = state.astype(jnp.bfloat16)
        pltpu.make_async_copy(out.at[rows], out_hbm.at[0, rows], sem).start()
    pltpu.make_async_copy(out, out_hbm.at[0], sem).wait()


def body(inputs, conv_weight, gate_weight, rate_param, pace):
    nsp = lax.axis_size("sp")
    ndp = lax.axis_size("dp")
    _, count, width = inputs.shape
    block = gate_weight.shape[-1]
    heads = width // block
    hl = heads // ndp
    lines = width // LANES
    f32, bf16 = jnp.float32, jnp.bfloat16
    hbm = pl.BlockSpec(memory_space=pltpu.HBM)
    dma = pltpu.SemaphoreType.DMA
    part_h, part_a, carry = pl.pallas_call(
        functools.partial(kernel, nsp, ndp, heads, block),
        out_shape=(
            pltpu.VMEM((lines, count, LANES), f32),
            pltpu.VMEM((lines, count, LANES), f32),
            pltpu.VMEM((lines, LANES), f32),
        ),
        in_specs=[hbm] * 5,
        out_specs=[pl.BlockSpec(memory_space=pltpu.VMEM)] * 3,
        scratch_shapes=[
            pltpu.VMEM((count, width), bf16),
            pltpu.VMEM(conv_weight.shape, bf16),
            pltpu.VMEM((2, heads, block, block), bf16),
            pltpu.VMEM((1, width), f32),
            pltpu.VMEM((1, count), f32),
            pltpu.VMEM((count, LANES), f32),
            pltpu.VMEM((count // SUB, SUB, LANES), f32),
            pltpu.VMEM((CONV, width), bf16),
            pltpu.VMEM((CONV, width), bf16),
            pltpu.VMEM((heads, count, block), f32),
            pltpu.VMEM((SUB, width), f32),
            pltpu.VMEM((heads, count, block), f32),
            pltpu.VMEM((heads, count, block), f32),
            pltpu.VMEM((heads, SUB, block), f32),
            pltpu.VMEM((heads, SUB, block), f32),
            pltpu.VMEM((heads, SUB, block), f32),
            pltpu.VMEM((heads, SUB, block), f32),
            pltpu.VMEM((heads, SUB, block), f32),
            pltpu.VMEM((heads, SUB, block), f32),
            pltpu.VMEM((block // LANES, count, LANES), f32),
            pltpu.VMEM((block // LANES, count, LANES), f32),
            pltpu.VMEM((2 * lines, LANES), f32),
            pltpu.VMEM((2 * lines, LANES), bf16),
            pltpu.VMEM((2 * lines * nsp, LANES), bf16),
            pltpu.SemaphoreType.REGULAR((2,)),
            pltpu.SemaphoreType.REGULAR,
            dma,
            dma((2,)),
            dma,
            dma((heads - hl,)),
            dma,
            dma,
            dma,
            dma,
        ],
        compiler_params=pltpu.CompilerParams(collective_id=0, has_side_effects=True),
    )(inputs, conv_weight, gate_weight, rate_param.reshape(1, width), pace)
    return pl.pallas_call(
        finish,
        out_shape=jax.ShapeDtypeStruct(inputs.shape, bf16),
        in_specs=[pl.BlockSpec(memory_space=pltpu.VMEM)] * 3,
        out_specs=hbm,
        scratch_shapes=[pltpu.VMEM((count, width), bf16), dma],
        compiler_params=pltpu.CompilerParams(vmem_limit_bytes=8 * 2**20),
    )(part_h, part_a, carry)


def solution(mesh):
    return jax.shard_map(
        body,
        mesh=mesh,
        in_specs=(P("dp", "sp", None), P(), P(None, "dp", None, None), P(), P("dp", None)),
        out_specs=P("dp", "sp", None),
        check_vma=False,
    )
```

```python
import functools
import math

import jax
import jax.numpy as jnp
from jax import lax
from jax.experimental import pallas as pl
from jax.experimental.pallas import tpu as pltpu
from jax.sharding import PartitionSpec as P

CONV = 4
EDGE = CONV - 1
gate_power = 8.0
SUB = 8
LANES = 128
TINY = 1.2e-38
LN2 = math.log(2.0)
LOG2E = 1.0 / LN2
SMALL = 0.015
ROW = 4
FIRST = 2
MESH = pl.DeviceIdType.MESH


def softplus_neg(rate):
    e = jnp.exp(-jnp.abs(rate))
    series = e * (1.0 + e * (-0.5 + e * (1.0 / 3.0 + e * (-0.25 + e * 0.2))))
    return jnp.maximum(-rate, 0.0) + jnp.where(e < 0.03, series, jnp.log(1.0 + e))


def kernel(
    nsp, ndp, heads, block,
    x_hbm, cw_hbm, w_hbm, rate_hbm, pace_hbm, part_h, part_a, carry,
    x, cw, w, rate, pace_row, pace_mat, pace_perm, last, halo,
    convs, conv0, hloc, acum, all_h, all_a, edge_h, edge_a, ex_h, ex_a, lay_h, lay_a, stage, send_buf, recv_buf,
    known, met, load_sem, map_sem, w_send, w_recv, halo_send, halo_recv, c_send, c_recv,
):
    me = lax.axis_index("sp")
    d = lax.axis_index("dp")
    count, width = x.shape
    steps = count // SUB
    hl = heads // ndp
    tiles = block // LANES
    lines = heads * tiles
    root = nsp - 1
    relay = nsp // 2 + 1 if nsp >= 2 * ROW else 0
    reach = nsp // 2 + ROW - 1
    near = 2
    scope = jax.named_scope

    first = pl.multiple_of(me * count, count)
    loads = [
        pltpu.make_async_copy(x_hbm.at[0], x, load_sem),
        pltpu.make_async_copy(cw_hbm, cw, load_sem),
        pltpu.make_async_copy(rate_hbm, rate, load_sem),
        pltpu.make_async_copy(pace_hbm.at[:, pl.ds(first, count)], pace_row, load_sem),
    ]
    map_loads = [
        pltpu.make_async_copy(w_hbm.at[:, own], w.at[:, own], map_sem.at[int(own >= FIRST)])
        for own in range(hl)
    ]
    for load in loads + map_loads:
        load.start()

    recv_buf[...] = jnp.zeros_like(recv_buf)

    barrier = pltpu.get_barrier_semaphore()

    def greet(there):
        pl.semaphore_signal(barrier, inc=1, device_id={"sp": there}, device_id_type=MESH)

    @pl.loop(d + 1, ndp)
    def _(o):
        pl.semaphore_signal(barrier, inc=1, device_id={"dp": o}, device_id_type=MESH)

    if root > 0:

        @pl.when(me > 0)
        def _():
            greet(me - 1)

    if root > 1:

        @pl.when(me < root - 1)
        def _():
            greet(root)

        @pl.when(me == root - 1)
        def _():
            greet(root)

    if relay:

        @pl.when(jnp.logical_and(d == 0, (me <= reach) & (me != relay) & (me != relay + 1)))
        def _():
            greet(relay)

    @pl.when(me == 0)
    def _():
        halo[...] = jnp.zeros_like(halo)

    def meet():
        expect = jnp.where(me == root, root if root > 1 else 0, min(root, 1))
        if relay:
            expect = jnp.where(jnp.logical_and(d == 0, me == relay), reach, expect)
        pl.semaphore_wait(barrier, d + expect)

    def meet_early():
        if root > 0:

            @pl.when(me == root)
            def _():
                meet()
                for there in range(root):
                    pl.semaphore_signal(known.at[0], inc=1, device_id={"sp": there}, device_id_type=MESH)

    def meet_maps():
        @pl.when(jnp.logical_and(me < max(root, 1), d > 0))
        def _():
            meet()

        @pl.loop(0, d)
        def _(o):
            pl.semaphore_signal(met, inc=1, device_id={"dp": o}, device_id_type=MESH)

        @pl.when(d < ndp - 1)
        def _():
            pl.semaphore_wait(met, ndp - 1 - d)

    def meet_halo():
        @pl.when(jnp.logical_and(me < root, d == 0))
        def _():
            meet()

            if relay:

                @pl.when(me == relay)
                def _():
                    for there in range(near):
                        pl.semaphore_signal(known.at[1], inc=1, device_id={"sp": there}, device_id_type=MESH)

    w_copies = []
    for slot in range(hl, heads):
        o, own = slot // hl, slot % hl
        w_copies.append(pltpu.make_async_remote_copy(
            src_ref=w.at[:, own],
            dst_ref=w.at[:, slot],
            send_sem=w_send,
            recv_sem=w_recv.at[slot - hl],
            device_id={"dp": lax.rem(d - o + ndp, ndp)},
            device_id_type=MESH,
        ))
    halo_copy = pltpu.make_async_remote_copy(
        src_ref=last,
        dst_ref=halo,
        send_sem=halo_send,
        recv_sem=halo_recv,
        device_id={"sp": lax.rem(me + 1, nsp)},
        device_id_type=MESH,
    )

    def carry_copy(src, dst, low=0):
        return pltpu.make_async_remote_copy(
            src_ref=send_buf.at[pl.ds(low, 2 * lines - low)],
            dst_ref=recv_buf.at[pl.ds(2 * lines * src + low, 2 * lines - low)],
            send_sem=c_send,
            recv_sem=c_recv,
            device_id={"sp": dst},
            device_id_type=MESH,
        )

    def carries(rows):
        block = recv_buf.at[pl.ds(0, rows)]
        return pltpu.make_async_remote_copy(
            src_ref=block,
            dst_ref=block,
            send_sem=c_send,
            recv_sem=c_recv,
            device_id={"sp": root - me},
            device_id_type=MESH,
        )

    row = lax.broadcasted_iota(jnp.int32, (count, count), 0)
    col = lax.broadcasted_iota(jnp.int32, (count, count), 1)
    gather = jnp.where(col == (row % SUB) * steps + row // SUB, 1.0, 0.0).astype(jnp.bfloat16)
    sub = lax.broadcasted_iota(jnp.int32, (SUB, block), 0)

    def columns(slot):
        return pl.ds(pl.multiple_of(lax.rem(d * hl + slot, heads) * block, block), block)

    def convolve(rows, here):
        taps = cw[:, here].astype(jnp.float32)
        taps = [jnp.broadcast_to(taps[k : k + 1], (SUB, block)) for k in range(CONV)]
        out = []
        for j in range(len(rows) - EDGE):
            total = taps[0] * rows[j]
            for k in range(1, CONV):
                total = total + taps[k] * rows[j + k]
            out.append(total)
        return jnp.concatenate(out, axis=0)

    def conv_main(slot):
        here = columns(slot)
        xp = jnp.dot(gather, x[:, here], preferred_element_type=jnp.float32)
        rows = [xp[SUB * j : SUB * (j + 1)] for j in range(steps)]
        rows = [pltpu.roll(rows[steps - EDGE + j], 1, 0) for j in range(EDGE)] + rows
        convs[slot] = convolve(rows, here)

    def gates(conv, slot, pace_of):
        conv = conv.astype(jnp.bfloat16)
        pre_r = jnp.dot(conv, w[0, slot], preferred_element_type=jnp.float32)
        pre_i = jnp.dot(conv, w[1, slot], preferred_element_type=jnp.float32)
        values = conv.astype(jnp.float32)
        factor = softplus_neg(rate[:, columns(slot)]) * (-gate_power / LN2)
        factor = jnp.broadcast_to(factor, (SUB, block))
        for j in range(conv.shape[0] // SUB):
            part = slice(SUB * j, SUB * (j + 1))
            pace_j = jnp.concatenate([pace_of(j)] * tiles, axis=1)
            r = 1.0 / (1.0 + jnp.exp2(pre_r[part] * -LOG2E))
            i = 1.0 / (1.0 + jnp.exp2(pre_i[part] * -LOG2E))
            n = pace_j * factor * r
            a = jnp.exp2(n)
            c = 2.0 * LN2
            series = n * (n * (n * (-(c**3) / 6) - c * c / 2) - c)
            gain = jnp.where(n > -SMALL, series, 1.0 - a * a)
            b = gain * lax.rsqrt(jnp.maximum(gain, TINY)) * i * values[part]
            yield a, b

    def prefix(h, total_a, shifts):
        for shift in shifts:
            inside = sub >= shift
            earlier_a = jnp.where(inside, pltpu.roll(total_a, shift, 0), 1.0)
            earlier_h = jnp.where(inside, pltpu.roll(h, shift, 0), 0.0)
            h = total_a * earlier_h + h
            total_a = total_a * earlier_a
        return h, total_a

    def main_slot(slot):
        for j, (a, b) in enumerate(gates(convs[slot], slot, lambda j: pace_perm[j])):
            if j == 0:
                h, total_a = b, a
            elif j == EDGE:
                h = jnp.where(sub == 0, b, a * h + b)
                total_a = jnp.where(sub == 0, a, total_a * a)
            else:
                h = a * h + b
                total_a = total_a * a
            place = slice(SUB * j, SUB * (j + 1))
            hloc[slot, place] = h
            acum[slot, place] = total_a
        h, total_a = prefix(h, total_a, (1, 2, 4))
        all_h[slot] = h
        all_a[slot] = total_a

    def conv_edge():
        own = pltpu.roll(x[:SUB, :].astype(jnp.float32), EDGE, 0)
        before = jnp.concatenate([halo[...].astype(jnp.float32)] * (SUB // CONV), axis=0)
        wide = lax.broadcasted_iota(jnp.int32, own.shape, 0)
        rows = jnp.where(wide < EDGE, before, own)
        taps = cw[...].astype(jnp.float32)
        total = taps[0:1] * rows
        for k in range(1, CONV):
            total = total + taps[k : k + 1] * pltpu.roll(rows, SUB - k, 0)
        conv0[...] = total

    def edge_slot(slot):
        (a, b), = gates(conv0[:, columns(slot)], slot, lambda j: pace_mat[:SUB, :])
        h, total_a = prefix(b, a, (1, 2))
        edge_h[slot] = h
        edge_a[slot] = total_a
        first_h = jnp.broadcast_to(h[EDGE - 1 : EDGE], (SUB, block))
        first_a = jnp.broadcast_to(total_a[EDGE - 1 : EDGE], (SUB, block))
        h, total_a = all_h[slot], all_a[slot]
        before_h = jnp.where(sub >= 1, pltpu.roll(h, 1, 0), 0.0)
        before_a = jnp.where(sub >= 1, pltpu.roll(total_a, 1, 0), 1.0)
        ex_h[slot] = before_h + before_a * first_h
        ex_a[slot] = before_a * first_a
        h = h + total_a * first_h
        log_a = jnp.log2(jnp.maximum(total_a * first_a, TINY))
        for t in range(tiles):
            lanes = slice(LANES * t, LANES * (t + 1))
            stage[pl.ds(slot * tiles + t, 1), :] = log_a[SUB - 1 :, lanes]
            stage[pl.ds(lines + slot * tiles + t, 1), :] = h[SUB - 1 :, lanes]

    with scope("meet_early"):
        meet_early()
    with scope("loads"):
        for load in loads:
            load.wait()
    last[...] = pltpu.roll(x[count - SUB :, :].astype(jnp.float32), EDGE, 0)[:CONV].astype(jnp.bfloat16)
    with scope("meet_maps"):
        meet_maps()
    with scope("maps_a"):
        for load in map_loads[:FIRST]:
            load.wait()
        for own in range(min(FIRST, hl)):
            for copy in w_copies[own::hl]:
                copy.start()

    def send_halo():
        if root > 0:

            @pl.when(me < root)
            def _():
                halo_copy.start()

    @pl.when(d > 0)
    def _():
        send_halo()

    spread = jnp.broadcast_to(pace_row[...], (LANES, count)).T
    pace_mat[...] = spread
    for j in range(steps):
        pace_perm[j] = pace_mat[pl.ds(j, SUB, stride=steps), :]

    with scope("conv_a"):
        for slot in range(hl // 4):
            conv_main(slot)
    with scope("meet_halo"):
        meet_halo()

    @pl.when(d == 0)
    def _():
        send_halo()

    with scope("conv_b"):
        for slot in range(hl // 4, hl):
            conv_main(slot)
    with scope("maps_b"):
        for load in map_loads[FIRST:]:
            load.wait()
        for own in range(FIRST, hl):
            for copy in w_copies[own::hl]:
                copy.start()
    def wait_halo():
        with scope("take_halo"):

            @pl.when(me > 0)
            def _():
                halo_copy.wait_recv()

    def wait_maps(turn):
        with scope("map%d" % turn[0]):
            for slot in turn:
                w_copies[slot - hl].wait_recv()

    def mains(turn, after=()):
        for slot in turn:
            main_slot(slot)
        for slot in after:
            conv_main(slot)

    def edges():
        conv_edge()
        for slot in range(heads):
            edge_slot(slot)
        send_buf[...] = stage[...].astype(jnp.bfloat16)

    own, rest = list(range(hl)), list(range(hl, heads))
    pair, single = rest[:2], [[slot] for slot in rest]

    def run(turns, ahead):
        for turn, after in zip(turns, ahead):
            wait_maps(turn)
            with scope("main%d" % turn[0]):
                mains(turn, after)

    with scope("main0"):
        mains(own, pair)

    @pl.when(d == 0)
    def _():
        run(([pair] if pair else []) + single[2:], single[2:] + [[]])
        wait_halo()
        with scope("edges"):
            edges()

    @pl.when(d > 0)
    def _():
        run(single[:-1], [[]] + single[2:])
        wait_halo()
        for turn in single[-1:]:
            wait_maps(turn)
        with scope("edges"):
            for turn in single[-1:]:
                mains(turn)
            edges()

    planes = -(-nsp // ROW)
    split = reach // ROW + 1 if relay else 0
    early = jnp.logical_and(me < near, d == 0) if relay else me < 0

    def all_in():
        if root > 0:

            @pl.when(me < root)
            def _():
                pl.semaphore_wait(known.at[0], 1)

    def send_first(low, high):
        for rest in reversed(range(ROW)):
            for plane in reversed(range(low, high)):
                if 0 < ROW * plane + rest < nsp:
                    carry_copy(0, ROW * plane + rest, lines).start()

    def send_rest(low, high):
        at = lax.rem(me, ROW)
        mid = 1 - lax.rem((at + 1) // 2, 2)
        rests = (ROW - 1 - at, mid, ROW - 1 - mid, at)
        for rest, way in zip(rests, (-1, 1, 1, -1)):
            for plane in range(low, high)[::way]:
                dst = ROW * plane + rest

                @pl.when(jnp.logical_and(me < dst, dst < nsp))
                def _(dst=dst):
                    carry_copy(me, dst).start()

    def send(low, high):
        @pl.when(me == 0)
        def _():
            send_first(low, high)

        @pl.when(me > 0)
        def _():
            send_rest(low, high)

    if relay:

        @pl.when(early)
        def _():
            pl.semaphore_wait(known.at[1], 1)
            send(0, split)

    with scope("all_in"):
        all_in()

    if relay:

        @pl.when(early)
        def _():
            send(split, planes)

    @pl.when(jnp.logical_not(early))
    def _():
        send(0, planes)

    with scope("lay"):

        @pl.loop(0, heads)
        def _(slot):
            before_h, before_a = ex_h[slot], ex_a[slot]
            for j in range(steps):
                place = slice(SUB * j, SUB * (j + 1))
                h = hloc[slot, place] + acum[slot, place] * before_h
                total_a = acum[slot, place] * before_a
                if j < EDGE:
                    h = jnp.where(sub == 0, edge_h[slot, j : j + 1], h)
                    total_a = jnp.where(sub == 0, edge_a[slot, j : j + 1], total_a)
                for t in range(tiles):
                    lanes = slice(LANES * t, LANES * (t + 1))
                    lay_h[t, place] = h[:, lanes]
                    lay_a[t, place] = total_a[:, lanes]
            for t in range(tiles):
                line = lax.rem(d * hl + slot, heads) * tiles + t
                for c in range(SUB):
                    for k in range(0, steps, SUB):
                        place = slice(steps * c + k, steps * c + k + SUB)
                        part_h[line, place] = lay_h[t, pl.ds(SUB * k + c, SUB, stride=SUB), :]
                        part_a[line, place] = lay_a[t, pl.ds(SUB * k + c, SUB, stride=SUB), :]

    with scope("sent"):
        for copy in w_copies:
            copy.wait_send()

        if root > 0:

            @pl.when(me < root)
            def _():
                halo_copy.wait_send()

        for many in range(1, nsp):

            @pl.when(root - me == many)
            def _(many=many):
                carries((2 if many < root else 1) * many * lines).wait_send()

    with scope("carry"):
        for many in range(1, nsp):

            @pl.when(me == many)
            def _(many=many):
                carries((2 * many - 1) * lines).wait_recv()

    with scope("finish"):
        start = jnp.zeros(carry.shape, jnp.float32)
        parts = []
        for src in range(root):
            got = recv_buf[2 * lines * src : 2 * lines * (src + 1)].astype(jnp.float32)
            parts.append((jnp.exp2(got[:lines]), got[lines:]))
        while len(parts) > 1:
            pairs = [(a0 * a1, a1 * h0 + h1) for (a0, h0), (a1, h1) in zip(parts[::2], parts[1::2])]
            parts = pairs + parts[len(parts) // 2 * 2 :]
        if parts:
            start = parts[0][1]
        for slot in range(heads):
            line = pl.multiple_of(lax.rem(d * hl + slot, heads) * tiles, tiles)
            carry[pl.ds(line, tiles), :] = start[slot * tiles : (slot + 1) * tiles]


def finish(part_h, part_a, carry, out_hbm, out, sem):
    lines = carry.shape[0]
    count = out.shape[0]
    for low in range(0, count, 2 * SUB):
        rows = slice(low, low + 2 * SUB)
        for line in range(lines):
            state = part_h[line, rows] + part_a[line, rows] * carry[line : line + 1, :]
            out[rows, LANES * line : LANES * (line + 1)] = state.astype(jnp.bfloat16)
        pltpu.make_async_copy(out.at[rows], out_hbm.at[0, rows], sem).start()
    pltpu.make_async_copy(out, out_hbm.at[0], sem).wait()


def body(inputs, conv_weight, gate_weight, rate_param, pace):
    nsp = lax.axis_size("sp")
    ndp = lax.axis_size("dp")
    _, count, width = inputs.shape
    block = gate_weight.shape[-1]
    heads = width // block
    hl = heads // ndp
    lines = width // LANES
    f32, bf16 = jnp.float32, jnp.bfloat16
    hbm = pl.BlockSpec(memory_space=pltpu.HBM)
    dma = pltpu.SemaphoreType.DMA
    part_h, part_a, carry = pl.pallas_call(
        functools.partial(kernel, nsp, ndp, heads, block),
        out_shape=(
            pltpu.VMEM((lines, count, LANES), f32),
            pltpu.VMEM((lines, count, LANES), f32),
            pltpu.VMEM((lines, LANES), f32),
        ),
        in_specs=[hbm] * 5,
        out_specs=[pl.BlockSpec(memory_space=pltpu.VMEM)] * 3,
        scratch_shapes=[
            pltpu.VMEM((count, width), bf16),
            pltpu.VMEM(conv_weight.shape, bf16),
            pltpu.VMEM((2, heads, block, block), bf16),
            pltpu.VMEM((1, width), f32),
            pltpu.VMEM((1, count), f32),
            pltpu.VMEM((count, LANES), f32),
            pltpu.VMEM((count // SUB, SUB, LANES), f32),
            pltpu.VMEM((CONV, width), bf16),
            pltpu.VMEM((CONV, width), bf16),
            pltpu.VMEM((heads, count, block), f32),
            pltpu.VMEM((SUB, width), f32),
            pltpu.VMEM((heads, count, block), f32),
            pltpu.VMEM((heads, count, block), f32),
            pltpu.VMEM((heads, SUB, block), f32),
            pltpu.VMEM((heads, SUB, block), f32),
            pltpu.VMEM((heads, SUB, block), f32),
            pltpu.VMEM((heads, SUB, block), f32),
            pltpu.VMEM((heads, SUB, block), f32),
            pltpu.VMEM((heads, SUB, block), f32),
            pltpu.VMEM((block // LANES, count, LANES), f32),
            pltpu.VMEM((block // LANES, count, LANES), f32),
            pltpu.VMEM((2 * lines, LANES), f32),
            pltpu.VMEM((2 * lines, LANES), bf16),
            pltpu.VMEM((2 * lines * nsp, LANES), bf16),
            pltpu.SemaphoreType.REGULAR((2,)),
            pltpu.SemaphoreType.REGULAR,
            dma,
            dma((2,)),
            dma,
            dma((heads - hl,)),
            dma,
            dma,
            dma,
            dma,
        ],
        compiler_params=pltpu.CompilerParams(collective_id=0, has_side_effects=True),
    )(inputs, conv_weight, gate_weight, rate_param.reshape(1, width), pace)
    return pl.pallas_call(
        finish,
        out_shape=jax.ShapeDtypeStruct(inputs.shape, bf16),
        in_specs=[pl.BlockSpec(memory_space=pltpu.VMEM)] * 3,
        out_specs=hbm,
        scratch_shapes=[pltpu.VMEM((count, width), bf16), dma],
        compiler_params=pltpu.CompilerParams(vmem_limit_bytes=8 * 2**20),
    )(part_h, part_a, carry)


def solution(mesh):
    return jax.shard_map(
        body,
        mesh=mesh,
        in_specs=(P("dp", "sp", None), P(), P(None, "dp", None, None), P(), P("dp", None)),
        out_specs=P("dp", "sp", None),
        check_vma=False,
    )
```

```python
import functools
import math

import jax
import jax.numpy as jnp
from jax import lax
from jax.experimental import pallas as pl
from jax.experimental.pallas import tpu as pltpu
from jax.sharding import PartitionSpec as P

CONV = 4
EDGE = CONV - 1
gate_power = 8.0
SUB = 8
LANES = 128
TINY = 1.2e-38
LN2 = math.log(2.0)
LOG2E = 1.0 / LN2
SMALL = 0.015
ROW = 4
FIRST = 2
MESH = pl.DeviceIdType.MESH


def softplus_neg(rate):
    e = jnp.exp(-jnp.abs(rate))
    series = e * (1.0 + e * (-0.5 + e * (1.0 / 3.0 + e * (-0.25 + e * 0.2))))
    return jnp.maximum(-rate, 0.0) + jnp.where(e < 0.03, series, jnp.log(1.0 + e))


def kernel(
    nsp, ndp, heads, block,
    x_hbm, cw_hbm, w_hbm, rate_hbm, pace_hbm, part_h, part_a, carry,
    x, cw, w, rate, factors, pace_row, pace_mat, pace_perm, last, halo,
    convs, conv0, hloc, acum, all_h, all_a, edge_h, edge_a, ex_h, ex_a, lay_h, lay_a, stage, send_buf, recv_buf,
    known, met, load_sem, map_sem, sent, w_recv, halo_recv, c_recv,
):
    me = lax.axis_index("sp")
    d = lax.axis_index("dp")
    count, width = x.shape
    steps = count // SUB
    hl = heads // ndp
    tiles = block // LANES
    lines = heads * tiles
    root = nsp - 1
    relay = nsp // 2 + 1 if nsp >= 2 * ROW else 0
    reach = nsp // 2 + ROW - 1
    near = 2
    scope = jax.named_scope

    first = pl.multiple_of(me * count, count)
    loads = [
        pltpu.make_async_copy(x_hbm.at[0], x, load_sem),
        pltpu.make_async_copy(cw_hbm, cw, load_sem),
        pltpu.make_async_copy(rate_hbm, rate, load_sem),
        pltpu.make_async_copy(pace_hbm.at[:, pl.ds(first, count)], pace_row, load_sem),
    ]
    map_loads = [
        pltpu.make_async_copy(w_hbm.at[:, own], w.at[:, own], map_sem.at[int(own >= FIRST)])
        for own in range(hl)
    ]
    for load in loads + map_loads:
        load.start()

    recv_buf[...] = jnp.zeros_like(recv_buf)

    barrier = pltpu.get_barrier_semaphore()

    def greet(there):
        pl.semaphore_signal(barrier, inc=1, device_id={"sp": there}, device_id_type=MESH)

    @pl.loop(d + 1, ndp)
    def _(o):
        pl.semaphore_signal(barrier, inc=1, device_id={"dp": o}, device_id_type=MESH)

    if root > 0:

        @pl.when(me > 0)
        def _():
            greet(me - 1)

    if root > 1:

        @pl.when(me < root - 1)
        def _():
            greet(root)

        @pl.when(me == root - 1)
        def _():
            greet(root)

    if relay:

        @pl.when(jnp.logical_and(d == 0, (me <= reach) & (me != relay) & (me != relay + 1)))
        def _():
            greet(relay)

    @pl.when(me == 0)
    def _():
        halo[...] = jnp.zeros_like(halo)

    def meet():
        expect = jnp.where(me == root, root if root > 1 else 0, min(root, 1))
        if relay:
            expect = jnp.where(jnp.logical_and(d == 0, me == relay), reach, expect)
        pl.semaphore_wait(barrier, d + expect)

    def meet_early():
        if root > 0:

            @pl.when(me == root)
            def _():
                meet()
                for there in range(root):
                    pl.semaphore_signal(known.at[0], inc=1, device_id={"sp": there}, device_id_type=MESH)

    def meet_maps():
        @pl.when(jnp.logical_and(me < max(root, 1), d > 0))
        def _():
            meet()

        @pl.loop(0, d)
        def _(o):
            pl.semaphore_signal(met, inc=1, device_id={"dp": o}, device_id_type=MESH)

        @pl.when(d < ndp - 1)
        def _():
            pl.semaphore_wait(met, ndp - 1 - d)

    def meet_halo():
        @pl.when(jnp.logical_and(me < root, d == 0))
        def _():
            meet()

            if relay:

                @pl.when(me == relay)
                def _():
                    for there in range(near):
                        pl.semaphore_signal(known.at[1], inc=1, device_id={"sp": there}, device_id_type=MESH)

    w_copies = []
    for slot in range(hl, heads):
        o, own = slot // hl, slot % hl
        w_copies.append(pltpu.make_async_remote_copy(
            src_ref=w.at[:, own],
            dst_ref=w.at[:, slot],
            send_sem=sent,
            recv_sem=w_recv.at[slot - hl],
            device_id={"dp": lax.rem(d - o + ndp, ndp)},
            device_id_type=MESH,
        ))
    halo_copy = pltpu.make_async_remote_copy(
        src_ref=last,
        dst_ref=halo,
        send_sem=sent,
        recv_sem=halo_recv,
        device_id={"sp": lax.rem(me + 1, nsp)},
        device_id_type=MESH,
    )

    def carry_copy(src, dst, low=0):
        return pltpu.make_async_remote_copy(
            src_ref=send_buf.at[pl.ds(low, 2 * lines - low)],
            dst_ref=recv_buf.at[pl.ds(2 * lines * src + low, 2 * lines - low)],
            send_sem=sent,
            recv_sem=c_recv,
            device_id={"sp": dst},
            device_id_type=MESH,
        )

    def carries(rows):
        block = recv_buf.at[pl.ds(0, rows)]
        return pltpu.make_async_remote_copy(
            src_ref=block,
            dst_ref=block,
            send_sem=sent,
            recv_sem=c_recv,
            device_id={"sp": root - me},
            device_id_type=MESH,
        )

    row = lax.broadcasted_iota(jnp.int32, (count, count), 0)
    col = lax.broadcasted_iota(jnp.int32, (count, count), 1)
    gather = jnp.where(col == (row % SUB) * steps + row // SUB, 1.0, 0.0).astype(jnp.bfloat16)
    sub = lax.broadcasted_iota(jnp.int32, (SUB, block), 0)

    def columns(slot):
        return pl.ds(pl.multiple_of(lax.rem(d * hl + slot, heads) * block, block), block)

    def convolve(rows, here):
        taps = cw[:, here].astype(jnp.float32)
        taps = [jnp.broadcast_to(taps[k : k + 1], (SUB, block)) for k in range(CONV)]
        out = []
        for j in range(len(rows) - EDGE):
            total = taps[0] * rows[j]
            for k in range(1, CONV):
                total = total + taps[k] * rows[j + k]
            out.append(total)
        return jnp.concatenate(out, axis=0)

    def conv_main(slot):
        here = columns(slot)
        xp = jnp.dot(gather, x[:, here], preferred_element_type=jnp.float32)
        rows = [xp[SUB * j : SUB * (j + 1)] for j in range(steps)]
        rows = [pltpu.roll(rows[steps - EDGE + j], 1, 0) for j in range(EDGE)] + rows
        convs[slot] = convolve(rows, here)

    def gates(conv, slot, pace_of):
        conv = conv.astype(jnp.bfloat16)
        pre_r = jnp.dot(conv, w[0, slot], preferred_element_type=jnp.float32)
        pre_i = jnp.dot(conv, w[1, slot], preferred_element_type=jnp.float32)
        values = conv.astype(jnp.float32)
        line = lax.rem(d * hl + slot, heads) * tiles
        factor = jnp.concatenate(
            [jnp.broadcast_to(factors[pl.ds(line + t, 1), :], (SUB, LANES)) for t in range(tiles)],
            axis=1,
        )
        for j in range(conv.shape[0] // SUB):
            part = slice(SUB * j, SUB * (j + 1))
            pace_j = jnp.concatenate([pace_of(j)] * tiles, axis=1)
            r = 1.0 / (1.0 + jnp.exp2(pre_r[part] * -LOG2E))
            i = 1.0 / (1.0 + jnp.exp2(pre_i[part] * -LOG2E))
            n = pace_j * factor * r
            a = jnp.exp2(n)
            c = 2.0 * LN2
            series = n * (n * (n * (-(c**3) / 6) - c * c / 2) - c)
            gain = jnp.where(n > -SMALL, series, 1.0 - a * a)
            b = gain * lax.rsqrt(jnp.maximum(gain, TINY)) * i * values[part]
            yield a, b

    def prefix(h, total_a, shifts):
        for shift in shifts:
            inside = sub >= shift
            earlier_a = jnp.where(inside, pltpu.roll(total_a, shift, 0), 1.0)
            earlier_h = jnp.where(inside, pltpu.roll(h, shift, 0), 0.0)
            h = total_a * earlier_h + h
            total_a = total_a * earlier_a
        return h, total_a

    def main_slot(slot):
        for j, (a, b) in enumerate(gates(convs[slot], slot, lambda j: pace_perm[j])):
            if j == 0:
                h, total_a = b, a
            elif j == EDGE:
                h = jnp.where(sub == 0, b, a * h + b)
                total_a = jnp.where(sub == 0, a, total_a * a)
            else:
                h = a * h + b
                total_a = total_a * a
            place = slice(SUB * j, SUB * (j + 1))
            hloc[slot, place] = h
            acum[slot, place] = total_a
        h, total_a = prefix(h, total_a, (1, 2, 4))
        all_h[slot] = h
        all_a[slot] = total_a

    def conv_edge():
        own = pltpu.roll(x[:SUB, :].astype(jnp.float32), EDGE, 0)
        before = jnp.concatenate([halo[...].astype(jnp.float32)] * (SUB // CONV), axis=0)
        wide = lax.broadcasted_iota(jnp.int32, own.shape, 0)
        rows = jnp.where(wide < EDGE, before, own)
        taps = cw[...].astype(jnp.float32)
        total = taps[0:1] * rows
        for k in range(1, CONV):
            total = total + taps[k : k + 1] * pltpu.roll(rows, SUB - k, 0)
        conv0[...] = total

    def edge_slot(slot):
        (a, b), = gates(conv0[:, columns(slot)], slot, lambda j: pace_mat[:SUB, :])
        h, total_a = prefix(b, a, (1, 2))
        edge_h[slot] = h
        edge_a[slot] = total_a
        first_h = jnp.broadcast_to(h[EDGE - 1 : EDGE], (SUB, block))
        first_a = jnp.broadcast_to(total_a[EDGE - 1 : EDGE], (SUB, block))
        h, total_a = all_h[slot], all_a[slot]
        before_h = jnp.where(sub >= 1, pltpu.roll(h, 1, 0), 0.0)
        before_a = jnp.where(sub >= 1, pltpu.roll(total_a, 1, 0), 1.0)
        ex_h[slot] = before_h + before_a * first_h
        ex_a[slot] = before_a * first_a
        h = h + total_a * first_h
        log_a = jnp.log2(jnp.maximum(total_a * first_a, TINY))
        for t in range(tiles):
            lanes = slice(LANES * t, LANES * (t + 1))
            stage[pl.ds(slot * tiles + t, 1), :] = log_a[SUB - 1 :, lanes]
            stage[pl.ds(lines + slot * tiles + t, 1), :] = h[SUB - 1 :, lanes]

    with scope("meet_early"):
        meet_early()
    with scope("loads"):
        for load in loads:
            load.wait()
    last[...] = pltpu.roll(x[count - SUB :, :].astype(jnp.float32), EDGE, 0)[:CONV].astype(jnp.bfloat16)
    with scope("meet_maps"):
        meet_maps()
    with scope("maps_a"):
        for load in map_loads[:FIRST]:
            load.wait()
        for own in range(min(FIRST, hl)):
            for copy in w_copies[own::hl]:
                copy.start()

    def send_halo():
        if root > 0:

            @pl.when(me < root)
            def _():
                halo_copy.start()

    @pl.when(d > 0)
    def _():
        send_halo()

    factors[...] = softplus_neg(rate[...]) * (-gate_power / LN2)
    spread = jnp.broadcast_to(pace_row[...], (LANES, count)).T
    pace_mat[...] = spread
    for j in range(steps):
        pace_perm[j] = pace_mat[pl.ds(j, SUB, stride=steps), :]

    with scope("conv_a"):
        for slot in range(hl // 4):
            conv_main(slot)
    with scope("meet_halo"):
        meet_halo()

    @pl.when(d == 0)
    def _():
        send_halo()

    with scope("conv_b"):
        for slot in range(hl // 4, hl):
            conv_main(slot)
    with scope("maps_b"):
        for load in map_loads[FIRST:]:
            load.wait()
        for own in range(FIRST, hl):
            for copy in w_copies[own::hl]:
                copy.start()
    def wait_halo():
        with scope("take_halo"):

            @pl.when(me > 0)
            def _():
                halo_copy.wait_recv()

    def wait_maps(turn):
        with scope("map%d" % turn[0]):
            for slot in turn:
                w_copies[slot - hl].wait_recv()

    def mains(turn, after=()):
        for slot in turn:
            main_slot(slot)
        for slot in after:
            conv_main(slot)

    def edges():
        conv_edge()
        for slot in range(heads):
            edge_slot(slot)
        send_buf[...] = stage[...].astype(jnp.bfloat16)

    own, rest = list(range(hl)), list(range(hl, heads))
    pair, single = rest[:2], [[slot] for slot in rest]

    def run(turns, ahead):
        for turn, after in zip(turns, ahead):
            wait_maps(turn)
            with scope("main%d" % turn[0]):
                mains(turn, after)

    with scope("main0"):
        mains(own, pair)

    @pl.when(d == 0)
    def _():
        run(([pair] if pair else []) + single[2:], single[2:] + [[]])
        wait_halo()
        with scope("edges"):
            edges()

    @pl.when(d > 0)
    def _():
        run(single[:-1], [[]] + single[2:])
        wait_halo()
        for turn in single[-1:]:
            wait_maps(turn)
        with scope("edges"):
            for turn in single[-1:]:
                mains(turn)
            edges()

    planes = -(-nsp // ROW)
    split = reach // ROW + 1 if relay else 0
    early = jnp.logical_and(me < near, d == 0) if relay else me < 0

    def all_in():
        if root > 0:

            @pl.when(me < root)
            def _():
                pl.semaphore_wait(known.at[0], 1)

    def send_first(low, high):
        for rest in reversed(range(ROW)):
            for plane in reversed(range(low, high)):
                if 0 < ROW * plane + rest < nsp:
                    carry_copy(0, ROW * plane + rest, lines).start()

    def send_rest(low, high):
        at = lax.rem(me, ROW)
        mid = 1 - lax.rem((at + 1) // 2, 2)
        rests = (ROW - 1 - at, mid, ROW - 1 - mid, at)
        for rest, way in zip(rests, (-1, 1, 1, -1)):
            for plane in range(low, high)[::way]:
                dst = ROW * plane + rest

                @pl.when(jnp.logical_and(me < dst, dst < nsp))
                def _(dst=dst):
                    carry_copy(me, dst).start()

    def send(low, high):
        @pl.when(me == 0)
        def _():
            send_first(low, high)

        @pl.when(me > 0)
        def _():
            send_rest(low, high)

    if relay:

        @pl.when(early)
        def _():
            pl.semaphore_wait(known.at[1], 1)
            send(0, split)

    with scope("all_in"):
        all_in()

    if relay:

        @pl.when(early)
        def _():
            send(split, planes)

    @pl.when(jnp.logical_not(early))
    def _():
        send(0, planes)

    with scope("lay"):

        @pl.loop(0, heads)
        def _(slot):
            before_h, before_a = ex_h[slot], ex_a[slot]
            for j in range(steps):
                place = slice(SUB * j, SUB * (j + 1))
                h = hloc[slot, place] + acum[slot, place] * before_h
                total_a = acum[slot, place] * before_a
                if j < EDGE:
                    h = jnp.where(sub == 0, edge_h[slot, j : j + 1], h)
                    total_a = jnp.where(sub == 0, edge_a[slot, j : j + 1], total_a)
                for t in range(tiles):
                    lanes = slice(LANES * t, LANES * (t + 1))
                    lay_h[t, place] = h[:, lanes]
                    lay_a[t, place] = total_a[:, lanes]
            for t in range(tiles):
                line = lax.rem(d * hl + slot, heads) * tiles + t
                for c in range(SUB):
                    for k in range(0, steps, SUB):
                        place = slice(steps * c + k, steps * c + k + SUB)
                        part_h[line, place] = lay_h[t, pl.ds(SUB * k + c, SUB, stride=SUB), :]
                        part_a[line, place] = lay_a[t, pl.ds(SUB * k + c, SUB, stride=SUB), :]

    with scope("sent"):
        for copy in w_copies:
            copy.wait_send()

        if root > 0:

            @pl.when(me < root)
            def _():
                halo_copy.wait_send()

        for many in range(1, nsp):

            @pl.when(root - me == many)
            def _(many=many):
                carries((2 if many < root else 1) * many * lines).wait_send()

    with scope("carry"):
        for many in range(1, nsp):

            @pl.when(me == many)
            def _(many=many):
                carries((2 * many - 1) * lines).wait_recv()

    with scope("finish"):
        start = jnp.zeros(carry.shape, jnp.float32)
        parts = []
        for src in range(root):
            got = recv_buf[2 * lines * src : 2 * lines * (src + 1)].astype(jnp.float32)
            parts.append((jnp.exp2(got[:lines]), got[lines:]))
        while len(parts) > 1:
            pairs = [(a0 * a1, a1 * h0 + h1) for (a0, h0), (a1, h1) in zip(parts[::2], parts[1::2])]
            parts = pairs + parts[len(parts) // 2 * 2 :]
        if parts:
            start = parts[0][1]
        for slot in range(heads):
            line = pl.multiple_of(lax.rem(d * hl + slot, heads) * tiles, tiles)
            carry[pl.ds(line, tiles), :] = start[slot * tiles : (slot + 1) * tiles]


def finish(part_h, part_a, carry, out_hbm, out, sem):
    lines = carry.shape[0]
    count = out.shape[0]
    for low in range(0, count, 2 * SUB):
        rows = slice(low, low + 2 * SUB)
        for line in range(lines):
            state = part_h[line, rows] + part_a[line, rows] * carry[line : line + 1, :]
            out[rows, LANES * line : LANES * (line + 1)] = state.astype(jnp.bfloat16)
        pltpu.make_async_copy(out.at[rows], out_hbm.at[0, rows], sem).start()
    pltpu.make_async_copy(out, out_hbm.at[0], sem).wait()


def body(inputs, conv_weight, gate_weight, rate_param, pace):
    nsp = lax.axis_size("sp")
    ndp = lax.axis_size("dp")
    _, count, width = inputs.shape
    block = gate_weight.shape[-1]
    heads = width // block
    hl = heads // ndp
    lines = width // LANES
    f32, bf16 = jnp.float32, jnp.bfloat16
    hbm = pl.BlockSpec(memory_space=pltpu.HBM)
    dma = pltpu.SemaphoreType.DMA
    part_h, part_a, carry = pl.pallas_call(
        functools.partial(kernel, nsp, ndp, heads, block),
        out_shape=(
            pltpu.VMEM((lines, count, LANES), f32),
            pltpu.VMEM((lines, count, LANES), f32),
            pltpu.VMEM((lines, LANES), f32),
        ),
        in_specs=[hbm] * 5,
        out_specs=[pl.BlockSpec(memory_space=pltpu.VMEM)] * 3,
        scratch_shapes=[
            pltpu.VMEM((count, width), bf16),
            pltpu.VMEM(conv_weight.shape, bf16),
            pltpu.VMEM((2, heads, block, block), bf16),
            pltpu.VMEM((lines, LANES), f32),
            pltpu.VMEM((lines, LANES), f32),
            pltpu.VMEM((1, count), f32),
            pltpu.VMEM((count, LANES), f32),
            pltpu.VMEM((count // SUB, SUB, LANES), f32),
            pltpu.VMEM((CONV, width), bf16),
            pltpu.VMEM((CONV, width), bf16),
            pltpu.VMEM((heads, count, block), f32),
            pltpu.VMEM((SUB, width), f32),
            pltpu.VMEM((heads, count, block), f32),
            pltpu.VMEM((heads, count, block), f32),
            pltpu.VMEM((heads, SUB, block), f32),
            pltpu.VMEM((heads, SUB, block), f32),
            pltpu.VMEM((heads, SUB, block), f32),
            pltpu.VMEM((heads, SUB, block), f32),
            pltpu.VMEM((heads, SUB, block), f32),
            pltpu.VMEM((heads, SUB, block), f32),
            pltpu.VMEM((block // LANES, count, LANES), f32),
            pltpu.VMEM((block // LANES, count, LANES), f32),
            pltpu.VMEM((2 * lines, LANES), f32),
            pltpu.VMEM((2 * lines, LANES), bf16),
            pltpu.VMEM((2 * lines * nsp, LANES), bf16),
            pltpu.SemaphoreType.REGULAR((2,)),
            pltpu.SemaphoreType.REGULAR,
            dma,
            dma((2,)),
            dma,
            dma((heads - hl,)),
            dma,
            dma,
        ],
        compiler_params=pltpu.CompilerParams(collective_id=0, has_side_effects=True),
    )(inputs, conv_weight, gate_weight, rate_param.reshape(lines, LANES), pace)
    return pl.pallas_call(
        finish,
        out_shape=jax.ShapeDtypeStruct(inputs.shape, bf16),
        in_specs=[pl.BlockSpec(memory_space=pltpu.VMEM)] * 3,
        out_specs=hbm,
        scratch_shapes=[pltpu.VMEM((count, width), bf16), dma],
        compiler_params=pltpu.CompilerParams(vmem_limit_bytes=8 * 2**20),
    )(part_h, part_a, carry)


def solution(mesh):
    return jax.shard_map(
        body,
        mesh=mesh,
        in_specs=(P("dp", "sp", None), P(), P(None, "dp", None, None), P(), P("dp", None)),
        out_specs=P("dp", "sp", None),
        check_vma=False,
    )
```

```python
import functools
import math

import jax
import jax.numpy as jnp
from jax import lax
from jax.experimental import pallas as pl
from jax.experimental.pallas import tpu as pltpu
from jax.sharding import PartitionSpec as P

CONV = 4
EDGE = CONV - 1
gate_power = 8.0
SUB = 8
LANES = 128
TINY = 1.2e-38
LN2 = math.log(2.0)
LOG2E = 1.0 / LN2
SMALL = 0.015
ROW = 4
FIRST = 2
MESH = pl.DeviceIdType.MESH


def softplus_neg(rate):
    e = jnp.exp(-jnp.abs(rate))
    series = e * (1.0 + e * (-0.5 + e * (1.0 / 3.0 + e * (-0.25 + e * 0.2))))
    return jnp.maximum(-rate, 0.0) + jnp.where(e < 0.03, series, jnp.log(1.0 + e))


def kernel(
    nsp, ndp, heads, block,
    x_hbm, cw_hbm, w_hbm, rate_hbm, pace_hbm, part_h, part_a, carry,
    x, cw, w, rate, factors, pace_row, pace_mat, pace_perm, last, halo,
    convs, conv0, hloc, acum, all_h, all_a, edge_h, edge_a, ex_h, ex_a, lay_h, lay_a, stage, send_buf, recv_buf,
    known, met, load_sem, map_sem, sent, w_recv, halo_recv, c_recv,
):
    me = lax.axis_index("sp")
    d = lax.axis_index("dp")
    count, width = x.shape
    steps = count // SUB
    hl = heads // ndp
    tiles = block // LANES
    lines = heads * tiles
    root = nsp - 1
    relay = nsp // 2 + 1 if nsp >= 2 * ROW else 0
    reach = nsp // 2 + ROW - 1
    near = 2
    scope = jax.named_scope

    first = pl.multiple_of(me * count, count)
    loads = [
        pltpu.make_async_copy(x_hbm.at[0], x, load_sem),
        pltpu.make_async_copy(cw_hbm, cw, load_sem),
        pltpu.make_async_copy(rate_hbm, rate, load_sem),
        pltpu.make_async_copy(pace_hbm.at[:, pl.ds(first, count)], pace_row, load_sem),
    ]
    map_loads = [
        pltpu.make_async_copy(w_hbm.at[:, own], w.at[:, own], map_sem.at[int(own >= FIRST)])
        for own in range(hl)
    ]
    for load in loads + map_loads:
        load.start()

    recv_buf[...] = jnp.zeros_like(recv_buf)

    barrier = pltpu.get_barrier_semaphore()

    def greet(there):
        pl.semaphore_signal(barrier, inc=1, device_id={"sp": there}, device_id_type=MESH)

    @pl.loop(d + 1, ndp)
    def _(o):
        pl.semaphore_signal(barrier, inc=1, device_id={"dp": o}, device_id_type=MESH)

    if root > 0:

        @pl.when(me > 0)
        def _():
            greet(me - 1)

    if root > 1:

        @pl.when(me < root - 1)
        def _():
            greet(root)

        @pl.when(me == root - 1)
        def _():
            greet(root)

    if relay:

        @pl.when(jnp.logical_and(d == 0, (me <= reach) & (me != relay) & (me != relay + 1)))
        def _():
            greet(relay)

    @pl.when(me == 0)
    def _():
        halo[...] = jnp.zeros_like(halo)

    def meet():
        expect = jnp.where(me == root, root if root > 1 else 0, min(root, 1))
        if relay:
            expect = jnp.where(jnp.logical_and(d == 0, me == relay), reach, expect)
        pl.semaphore_wait(barrier, d + expect)

    def meet_early():
        if root > 0:

            @pl.when(me == root)
            def _():
                meet()
                for there in range(root):
                    pl.semaphore_signal(known.at[0], inc=1, device_id={"sp": there}, device_id_type=MESH)

    def meet_maps():
        @pl.when(jnp.logical_and(me < max(root, 1), d > 0))
        def _():
            meet()

        @pl.loop(0, d)
        def _(o):
            pl.semaphore_signal(met, inc=1, device_id={"dp": o}, device_id_type=MESH)

        @pl.when(d < ndp - 1)
        def _():
            pl.semaphore_wait(met, ndp - 1 - d)

    def meet_halo():
        @pl.when(jnp.logical_and(me < root, d == 0))
        def _():
            meet()

            if relay:

                @pl.when(me == relay)
                def _():
                    for there in range(near):
                        pl.semaphore_signal(known.at[1], inc=1, device_id={"sp": there}, device_id_type=MESH)

    w_copies = []
    for slot in range(hl, heads):
        o, own = slot // hl, slot % hl
        w_copies.append(pltpu.make_async_remote_copy(
            src_ref=w.at[:, own],
            dst_ref=w.at[:, slot],
            send_sem=sent,
            recv_sem=w_recv.at[slot - hl],
            device_id={"dp": lax.rem(d - o + ndp, ndp)},
            device_id_type=MESH,
        ))
    halo_copy = pltpu.make_async_remote_copy(
        src_ref=last,
        dst_ref=halo,
        send_sem=sent,
        recv_sem=halo_recv,
        device_id={"sp": lax.rem(me + 1, nsp)},
        device_id_type=MESH,
    )

    def carry_copy(src, dst, low=0):
        return pltpu.make_async_remote_copy(
            src_ref=send_buf.at[pl.ds(low, 2 * lines - low)],
            dst_ref=recv_buf.at[pl.ds(2 * lines * src + low, 2 * lines - low)],
            send_sem=sent,
            recv_sem=c_recv,
            device_id={"sp": dst},
            device_id_type=MESH,
        )

    def carries(rows):
        block = recv_buf.at[pl.ds(0, rows)]
        return pltpu.make_async_remote_copy(
            src_ref=block,
            dst_ref=block,
            send_sem=sent,
            recv_sem=c_recv,
            device_id={"sp": root - me},
            device_id_type=MESH,
        )

    row = lax.broadcasted_iota(jnp.int32, (count, count), 0)
    col = lax.broadcasted_iota(jnp.int32, (count, count), 1)
    gather = jnp.where(col == (row % SUB) * steps + row // SUB, 1.0, 0.0).astype(jnp.bfloat16)
    sub = lax.broadcasted_iota(jnp.int32, (SUB, block), 0)

    def columns(slot):
        return pl.ds(pl.multiple_of(lax.rem(d * hl + slot, heads) * block, block), block)

    def convolve(rows, here):
        taps = cw[:, here].astype(jnp.float32)
        taps = [jnp.broadcast_to(taps[k : k + 1], (SUB, block)) for k in range(CONV)]
        out = []
        for j in range(len(rows) - EDGE):
            total = taps[0] * rows[j]
            for k in range(1, CONV):
                total = total + taps[k] * rows[j + k]
            out.append(total)
        return jnp.concatenate(out, axis=0)

    def conv_main(slot):
        here = columns(slot)
        xp = jnp.dot(gather, x[:, here], preferred_element_type=jnp.float32)
        rows = [xp[SUB * j : SUB * (j + 1)] for j in range(steps)]
        rows = [pltpu.roll(rows[steps - EDGE + j], 1, 0) for j in range(EDGE)] + rows
        convs[slot] = convolve(rows, here)

    def gates(conv, slot, pace_of):
        conv = conv.astype(jnp.bfloat16)
        pre_r = jnp.dot(conv, w[0, slot], preferred_element_type=jnp.float32)
        pre_i = jnp.dot(conv, w[1, slot], preferred_element_type=jnp.float32)
        values = conv.astype(jnp.float32)
        line = lax.rem(d * hl + slot, heads) * tiles
        factor = jnp.concatenate(
            [jnp.broadcast_to(factors[pl.ds(line + t, 1), :], (SUB, LANES)) for t in range(tiles)],
            axis=1,
        )
        for j in range(conv.shape[0] // SUB):
            part = slice(SUB * j, SUB * (j + 1))
            pace_j = jnp.concatenate([pace_of(j)] * tiles, axis=1)
            r = 1.0 / (1.0 + jnp.exp2(pre_r[part] * -LOG2E))
            i = 1.0 / (1.0 + jnp.exp2(pre_i[part] * -LOG2E))
            n = pace_j * factor * r
            a = jnp.exp2(n)
            c = 2.0 * LN2
            series = n * (n * (n * (-(c**3) / 6) - c * c / 2) - c)
            gain = jnp.where(n > -SMALL, series, 1.0 - a * a)
            b = gain * lax.rsqrt(jnp.maximum(gain, TINY)) * i * values[part]
            yield a, b

    def prefix(h, total_a, shifts):
        for shift in shifts:
            inside = sub >= shift
            earlier_a = jnp.where(inside, pltpu.roll(total_a, shift, 0), 1.0)
            earlier_h = jnp.where(inside, pltpu.roll(h, shift, 0), 0.0)
            h = total_a * earlier_h + h
            total_a = total_a * earlier_a
        return h, total_a

    def main_slot(slot):
        for j, (a, b) in enumerate(gates(convs[slot], slot, lambda j: pace_perm[j])):
            if j == 0:
                h, total_a = b, a
            elif j == EDGE:
                h = jnp.where(sub == 0, b, a * h + b)
                total_a = jnp.where(sub == 0, a, total_a * a)
            else:
                h = a * h + b
                total_a = total_a * a
            place = slice(SUB * j, SUB * (j + 1))
            hloc[slot, place] = h
            acum[slot, place] = total_a
        h, total_a = prefix(h, total_a, (1, 2, 4))
        all_h[slot] = h
        all_a[slot] = total_a

    def conv_edge():
        own = pltpu.roll(x[:SUB, :].astype(jnp.float32), EDGE, 0)
        before = jnp.concatenate([halo[...].astype(jnp.float32)] * (SUB // CONV), axis=0)
        wide = lax.broadcasted_iota(jnp.int32, own.shape, 0)
        rows = jnp.where(wide < EDGE, before, own)
        taps = cw[...].astype(jnp.float32)
        total = taps[0:1] * rows
        for k in range(1, CONV):
            total = total + taps[k : k + 1] * pltpu.roll(rows, SUB - k, 0)
        conv0[...] = total

    def edge_slot(slot):
        (a, b), = gates(conv0[:, columns(slot)], slot, lambda j: pace_mat[:SUB, :])
        h, total_a = prefix(b, a, (1, 2))
        edge_h[slot] = h
        edge_a[slot] = total_a
        first_h = jnp.broadcast_to(h[EDGE - 1 : EDGE], (SUB, block))
        first_a = jnp.broadcast_to(total_a[EDGE - 1 : EDGE], (SUB, block))
        h, total_a = all_h[slot], all_a[slot]
        before_h = jnp.where(sub >= 1, pltpu.roll(h, 1, 0), 0.0)
        before_a = jnp.where(sub >= 1, pltpu.roll(total_a, 1, 0), 1.0)
        ex_h[slot] = before_h + before_a * first_h
        ex_a[slot] = before_a * first_a
        h = h + total_a * first_h
        log_a = jnp.log2(jnp.maximum(total_a * first_a, TINY))
        for t in range(tiles):
            lanes = slice(LANES * t, LANES * (t + 1))
            stage[pl.ds(slot * tiles + t, 1), :] = log_a[SUB - 1 :, lanes]
            stage[pl.ds(lines + slot * tiles + t, 1), :] = h[SUB - 1 :, lanes]

    with scope("meet_early"):
        meet_early()
    with scope("loads"):
        for load in loads:
            load.wait()
    last[...] = pltpu.roll(x[count - SUB :, :].astype(jnp.float32), EDGE, 0)[:CONV].astype(jnp.bfloat16)
    with scope("meet_maps"):
        meet_maps()
    with scope("maps_a"):
        for load in map_loads[:FIRST]:
            load.wait()
        for own in range(min(FIRST, hl)):
            for copy in w_copies[own::hl]:
                copy.start()

    def send_halo():
        if root > 0:

            @pl.when(me < root)
            def _():
                halo_copy.start()

    @pl.when(d > 0)
    def _():
        send_halo()

    factors[...] = softplus_neg(rate[...]) * (-gate_power / LN2)
    spread = jnp.broadcast_to(pace_row[...], (LANES, count)).T
    pace_mat[...] = spread
    for j in range(steps):
        pace_perm[j] = pace_mat[pl.ds(j, SUB, stride=steps), :]

    with scope("conv_a"):
        for slot in range(hl // 4):
            conv_main(slot)
    with scope("meet_halo"):
        meet_halo()

    @pl.when(d == 0)
    def _():
        send_halo()

    with scope("conv_b"):
        for slot in range(hl // 4, hl):
            conv_main(slot)
    with scope("maps_b"):
        for load in map_loads[FIRST:]:
            load.wait()
        for own in range(FIRST, hl):
            for copy in w_copies[own::hl]:
                copy.start()
    def wait_halo():
        with scope("take_halo"):

            @pl.when(me > 0)
            def _():
                halo_copy.wait_recv()

    def wait_maps(turn):
        with scope("map%d" % turn[0]):
            for slot in turn:
                w_copies[slot - hl].wait_recv()

    def mains(turn, after=()):
        for slot in turn:
            main_slot(slot)
        for slot in after:
            conv_main(slot)

    def edges():
        conv_edge()
        for slot in range(heads):
            edge_slot(slot)
        send_buf[...] = stage[...].astype(jnp.bfloat16)

    own, rest = list(range(hl)), list(range(hl, heads))
    pair, single = rest[:2], [[slot] for slot in rest]

    def run(turns, ahead):
        for turn, after in zip(turns, ahead):
            wait_maps(turn)
            with scope("main%d" % turn[0]):
                mains(turn, after)

    with scope("main0"):
        mains(own, pair)

    @pl.when(d == 0)
    def _():
        run(([pair] if pair else []) + single[2:], single[2:] + [[]])
        wait_halo()
        with scope("edges"):
            edges()

    @pl.when(d > 0)
    def _():
        run(single[:-1], [[]] + single[2:])
        wait_halo()
        for turn in single[-1:]:
            wait_maps(turn)
        with scope("edges"):
            for turn in single[-1:]:
                mains(turn)
            edges()

    planes = -(-nsp // ROW)
    split = reach // ROW + 1 if relay else 0
    early = jnp.logical_and(me < near, d == 0) if relay else me < 0

    def all_in():
        if root > 0:

            @pl.when(me < root)
            def _():
                pl.semaphore_wait(known.at[0], 1)

    def send_first(low, high):
        for rest in reversed(range(ROW)):
            for plane in reversed(range(low, high)):
                if 0 < ROW * plane + rest < nsp:
                    carry_copy(0, ROW * plane + rest, lines).start()

    def send_rest(low, high):
        at = lax.rem(me, ROW)
        mid = 1 - lax.rem((at + 1) // 2, 2)
        rests = (ROW - 1 - at, mid, ROW - 1 - mid, at)
        for rest, way in zip(rests, (-1, 1, 1, 1)):
            for plane in range(low, high)[::way]:
                dst = ROW * plane + rest

                @pl.when(jnp.logical_and(me < dst, dst < nsp))
                def _(dst=dst):
                    carry_copy(me, dst).start()

    def send(low, high):
        @pl.when(me == 0)
        def _():
            send_first(low, high)

        @pl.when(me > 0)
        def _():
            send_rest(low, high)

    if relay:

        @pl.when(early)
        def _():
            pl.semaphore_wait(known.at[1], 1)
            send(0, split)

    with scope("all_in"):
        all_in()

    if relay:

        @pl.when(early)
        def _():
            send(split, planes)

    @pl.when(jnp.logical_not(early))
    def _():
        send(0, planes)

    with scope("lay"):

        @pl.loop(0, heads)
        def _(slot):
            before_h, before_a = ex_h[slot], ex_a[slot]
            for j in range(steps):
                place = slice(SUB * j, SUB * (j + 1))
                h = hloc[slot, place] + acum[slot, place] * before_h
                total_a = acum[slot, place] * before_a
                if j < EDGE:
                    h = jnp.where(sub == 0, edge_h[slot, j : j + 1], h)
                    total_a = jnp.where(sub == 0, edge_a[slot, j : j + 1], total_a)
                for t in range(tiles):
                    lanes = slice(LANES * t, LANES * (t + 1))
                    lay_h[t, place] = h[:, lanes]
                    lay_a[t, place] = total_a[:, lanes]
            for t in range(tiles):
                line = lax.rem(d * hl + slot, heads) * tiles + t
                for c in range(SUB):
                    for k in range(0, steps, SUB):
                        place = slice(steps * c + k, steps * c + k + SUB)
                        part_h[line, place] = lay_h[t, pl.ds(SUB * k + c, SUB, stride=SUB), :]
                        part_a[line, place] = lay_a[t, pl.ds(SUB * k + c, SUB, stride=SUB), :]

    with scope("sent"):
        for copy in w_copies:
            copy.wait_send()

        if root > 0:

            @pl.when(me < root)
            def _():
                halo_copy.wait_send()

        for many in range(1, nsp):

            @pl.when(root - me == many)
            def _(many=many):
                carries((2 if many < root else 1) * many * lines).wait_send()

    with scope("carry"):
        for many in range(1, nsp):

            @pl.when(me == many)
            def _(many=many):
                carries((2 * many - 1) * lines).wait_recv()

    with scope("finish"):
        start = jnp.zeros(carry.shape, jnp.float32)
        parts = []
        for src in range(root):
            got = recv_buf[2 * lines * src : 2 * lines * (src + 1)].astype(jnp.float32)
            parts.append((jnp.exp2(got[:lines]), got[lines:]))
        while len(parts) > 1:
            pairs = [(a0 * a1, a1 * h0 + h1) for (a0, h0), (a1, h1) in zip(parts[::2], parts[1::2])]
            parts = pairs + parts[len(parts) // 2 * 2 :]
        if parts:
            start = parts[0][1]
        for slot in range(heads):
            line = pl.multiple_of(lax.rem(d * hl + slot, heads) * tiles, tiles)
            carry[pl.ds(line, tiles), :] = start[slot * tiles : (slot + 1) * tiles]


def finish(part_h, part_a, carry, out_hbm, out, sem):
    lines = carry.shape[0]
    count = out.shape[0]
    for low in range(0, count, 2 * SUB):
        rows = slice(low, low + 2 * SUB)
        for line in range(lines):
            state = part_h[line, rows] + part_a[line, rows] * carry[line : line + 1, :]
            out[rows, LANES * line : LANES * (line + 1)] = state.astype(jnp.bfloat16)
        pltpu.make_async_copy(out.at[rows], out_hbm.at[0, rows], sem).start()
    pltpu.make_async_copy(out, out_hbm.at[0], sem).wait()


def body(inputs, conv_weight, gate_weight, rate_param, pace):
    nsp = lax.axis_size("sp")
    ndp = lax.axis_size("dp")
    _, count, width = inputs.shape
    block = gate_weight.shape[-1]
    heads = width // block
    hl = heads // ndp
    lines = width // LANES
    f32, bf16 = jnp.float32, jnp.bfloat16
    hbm = pl.BlockSpec(memory_space=pltpu.HBM)
    dma = pltpu.SemaphoreType.DMA
    part_h, part_a, carry = pl.pallas_call(
        functools.partial(kernel, nsp, ndp, heads, block),
        out_shape=(
            pltpu.VMEM((lines, count, LANES), f32),
            pltpu.VMEM((lines, count, LANES), f32),
            pltpu.VMEM((lines, LANES), f32),
        ),
        in_specs=[hbm] * 5,
        out_specs=[pl.BlockSpec(memory_space=pltpu.VMEM)] * 3,
        scratch_shapes=[
            pltpu.VMEM((count, width), bf16),
            pltpu.VMEM(conv_weight.shape, bf16),
            pltpu.VMEM((2, heads, block, block), bf16),
            pltpu.VMEM((lines, LANES), f32),
            pltpu.VMEM((lines, LANES), f32),
            pltpu.VMEM((1, count), f32),
            pltpu.VMEM((count, LANES), f32),
            pltpu.VMEM((count // SUB, SUB, LANES), f32),
            pltpu.VMEM((CONV, width), bf16),
            pltpu.VMEM((CONV, width), bf16),
            pltpu.VMEM((heads, count, block), f32),
            pltpu.VMEM((SUB, width), f32),
            pltpu.VMEM((heads, count, block), f32),
            pltpu.VMEM((heads, count, block), f32),
            pltpu.VMEM((heads, SUB, block), f32),
            pltpu.VMEM((heads, SUB, block), f32),
            pltpu.VMEM((heads, SUB, block), f32),
            pltpu.VMEM((heads, SUB, block), f32),
            pltpu.VMEM((heads, SUB, block), f32),
            pltpu.VMEM((heads, SUB, block), f32),
            pltpu.VMEM((block // LANES, count, LANES), f32),
            pltpu.VMEM((block // LANES, count, LANES), f32),
            pltpu.VMEM((2 * lines, LANES), f32),
            pltpu.VMEM((2 * lines, LANES), bf16),
            pltpu.VMEM((2 * lines * nsp, LANES), bf16),
            pltpu.SemaphoreType.REGULAR((2,)),
            pltpu.SemaphoreType.REGULAR,
            dma,
            dma((2,)),
            dma,
            dma((heads - hl,)),
            dma,
            dma,
        ],
        compiler_params=pltpu.CompilerParams(collective_id=0, has_side_effects=True),
    )(inputs, conv_weight, gate_weight, rate_param.reshape(lines, LANES), pace)
    return pl.pallas_call(
        finish,
        out_shape=jax.ShapeDtypeStruct(inputs.shape, bf16),
        in_specs=[pl.BlockSpec(memory_space=pltpu.VMEM)] * 3,
        out_specs=hbm,
        scratch_shapes=[pltpu.VMEM((count, width), bf16), dma],
        compiler_params=pltpu.CompilerParams(vmem_limit_bytes=8 * 2**20),
    )(part_h, part_a, carry)


def solution(mesh):
    return jax.shard_map(
        body,
        mesh=mesh,
        in_specs=(P("dp", "sp", None), P(), P(None, "dp", None, None), P(), P("dp", None)),
        out_specs=P("dp", "sp", None),
        check_vma=False,
    )
```

```python
import functools
import math

import jax
import jax.numpy as jnp
from jax import lax
from jax.experimental import pallas as pl
from jax.experimental.pallas import tpu as pltpu
from jax.sharding import PartitionSpec as P

CONV = 4
EDGE = CONV - 1
gate_power = 8.0
SUB = 8
LANES = 128
TINY = 1.2e-38
LN2 = math.log(2.0)
LOG2E = 1.0 / LN2
SMALL = 0.015
ROW = 4
FIRST = 2
MESH = pl.DeviceIdType.MESH


def softplus_neg(rate):
    e = jnp.exp(-jnp.abs(rate))
    series = e * (1.0 + e * (-0.5 + e * (1.0 / 3.0 + e * (-0.25 + e * 0.2))))
    return jnp.maximum(-rate, 0.0) + jnp.where(e < 0.03, series, jnp.log(1.0 + e))


def kernel(
    nsp, ndp, heads, block,
    x_hbm, cw_hbm, w_hbm, rate_hbm, pace_hbm, part_h, part_a, carry,
    x, cw, w, rate, factors, pace_row, pace_mat, pace_perm, last, halo,
    convs, conv0, hloc, acum, all_h, all_a, edge_h, edge_a, ex_h, ex_a, lay_h, lay_a, stage, send_buf, recv_buf,
    known, met, load_sem, map_sem, sent, w_recv, halo_recv, c_recv,
):
    me = lax.axis_index("sp")
    d = lax.axis_index("dp")
    count, width = x.shape
    steps = count // SUB
    hl = heads // ndp
    tiles = block // LANES
    lines = heads * tiles
    root = nsp - 1
    relay = nsp // 2 + 1 if nsp >= 2 * ROW else 0
    reach = nsp // 2 + ROW - 1
    near = 2
    scope = jax.named_scope

    first = pl.multiple_of(me * count, count)
    loads = [
        pltpu.make_async_copy(x_hbm.at[0], x, load_sem),
        pltpu.make_async_copy(cw_hbm, cw, load_sem),
        pltpu.make_async_copy(rate_hbm, rate, load_sem),
        pltpu.make_async_copy(pace_hbm.at[:, pl.ds(first, count)], pace_row, load_sem),
    ]
    map_loads = [
        pltpu.make_async_copy(w_hbm.at[:, own], w.at[:, own], map_sem.at[int(own >= FIRST)])
        for own in range(hl)
    ]
    for load in loads[:1] + map_loads[:FIRST]:
        load.start()

    recv_buf[...] = jnp.zeros_like(recv_buf)

    barrier = pltpu.get_barrier_semaphore()

    def greet(there):
        pl.semaphore_signal(barrier, inc=1, device_id={"sp": there}, device_id_type=MESH)

    @pl.loop(d + 1, ndp)
    def _(o):
        pl.semaphore_signal(barrier, inc=1, device_id={"dp": o}, device_id_type=MESH)

    if root > 0:

        @pl.when(me > 0)
        def _():
            greet(me - 1)

    if root > 1:

        @pl.when(me < root - 1)
        def _():
            greet(root)

        @pl.when(me == root - 1)
        def _():
            greet(root)

    if relay:

        @pl.when(jnp.logical_and(d == 0, (me <= reach) & (me != relay) & (me != relay + 1)))
        def _():
            greet(relay)

    for load in loads[1:] + map_loads[FIRST:]:
        load.start()

    @pl.when(me == 0)
    def _():
        halo[...] = jnp.zeros_like(halo)

    def meet():
        expect = jnp.where(me == root, root if root > 1 else 0, min(root, 1))
        if relay:
            expect = jnp.where(jnp.logical_and(d == 0, me == relay), reach, expect)
        pl.semaphore_wait(barrier, d + expect)

    def meet_early():
        if root > 0:

            @pl.when(me == root)
            def _():
                meet()
                for there in range(root):
                    pl.semaphore_signal(known.at[0], inc=1, device_id={"sp": there}, device_id_type=MESH)

    def meet_maps():
        @pl.when(jnp.logical_and(me < max(root, 1), d > 0))
        def _():
            meet()

        @pl.loop(0, d)
        def _(o):
            pl.semaphore_signal(met, inc=1, device_id={"dp": o}, device_id_type=MESH)

        @pl.when(d < ndp - 1)
        def _():
            pl.semaphore_wait(met, ndp - 1 - d)

    def meet_halo():
        @pl.when(jnp.logical_and(me < root, d == 0))
        def _():
            meet()

            if relay:

                @pl.when(me == relay)
                def _():
                    for there in range(near):
                        pl.semaphore_signal(known.at[1], inc=1, device_id={"sp": there}, device_id_type=MESH)

    w_copies = []
    for slot in range(hl, heads):
        o, own = slot // hl, slot % hl
        w_copies.append(pltpu.make_async_remote_copy(
            src_ref=w.at[:, own],
            dst_ref=w.at[:, slot],
            send_sem=sent,
            recv_sem=w_recv.at[slot - hl],
            device_id={"dp": lax.rem(d - o + ndp, ndp)},
            device_id_type=MESH,
        ))
    halo_copy = pltpu.make_async_remote_copy(
        src_ref=last,
        dst_ref=halo,
        send_sem=sent,
        recv_sem=halo_recv,
        device_id={"sp": lax.rem(me + 1, nsp)},
        device_id_type=MESH,
    )

    def carry_copy(src, dst, low=0):
        return pltpu.make_async_remote_copy(
            src_ref=send_buf.at[pl.ds(low, 2 * lines - low)],
            dst_ref=recv_buf.at[pl.ds(2 * lines * src + low, 2 * lines - low)],
            send_sem=sent,
            recv_sem=c_recv,
            device_id={"sp": dst},
            device_id_type=MESH,
        )

    def carries(rows):
        block = recv_buf.at[pl.ds(0, rows)]
        return pltpu.make_async_remote_copy(
            src_ref=block,
            dst_ref=block,
            send_sem=sent,
            recv_sem=c_recv,
            device_id={"sp": root - me},
            device_id_type=MESH,
        )

    row = lax.broadcasted_iota(jnp.int32, (count, count), 0)
    col = lax.broadcasted_iota(jnp.int32, (count, count), 1)
    gather = jnp.where(col == (row % SUB) * steps + row // SUB, 1.0, 0.0).astype(jnp.bfloat16)
    sub = lax.broadcasted_iota(jnp.int32, (SUB, block), 0)

    def columns(slot):
        return pl.ds(pl.multiple_of(lax.rem(d * hl + slot, heads) * block, block), block)

    def convolve(rows, here):
        taps = cw[:, here].astype(jnp.float32)
        taps = [jnp.broadcast_to(taps[k : k + 1], (SUB, block)) for k in range(CONV)]
        out = []
        for j in range(len(rows) - EDGE):
            total = taps[0] * rows[j]
            for k in range(1, CONV):
                total = total + taps[k] * rows[j + k]
            out.append(total)
        return jnp.concatenate(out, axis=0)

    def conv_main(slot):
        here = columns(slot)
        xp = jnp.dot(gather, x[:, here], preferred_element_type=jnp.float32)
        rows = [xp[SUB * j : SUB * (j + 1)] for j in range(steps)]
        rows = [pltpu.roll(rows[steps - EDGE + j], 1, 0) for j in range(EDGE)] + rows
        convs[slot] = convolve(rows, here)

    def gates(conv, slot, pace_of):
        conv = conv.astype(jnp.bfloat16)
        pre_r = jnp.dot(conv, w[0, slot], preferred_element_type=jnp.float32)
        pre_i = jnp.dot(conv, w[1, slot], preferred_element_type=jnp.float32)
        values = conv.astype(jnp.float32)
        line = lax.rem(d * hl + slot, heads) * tiles
        factor = jnp.concatenate(
            [jnp.broadcast_to(factors[pl.ds(line + t, 1), :], (SUB, LANES)) for t in range(tiles)],
            axis=1,
        )
        for j in range(conv.shape[0] // SUB):
            part = slice(SUB * j, SUB * (j + 1))
            pace_j = jnp.concatenate([pace_of(j)] * tiles, axis=1)
            r = 1.0 / (1.0 + jnp.exp2(pre_r[part] * -LOG2E))
            i = 1.0 / (1.0 + jnp.exp2(pre_i[part] * -LOG2E))
            n = pace_j * factor * r
            a = jnp.exp2(n)
            c = 2.0 * LN2
            series = n * (n * (n * (-(c**3) / 6) - c * c / 2) - c)
            gain = jnp.where(n > -SMALL, series, 1.0 - a * a)
            b = gain * lax.rsqrt(jnp.maximum(gain, TINY)) * i * values[part]
            yield a, b

    def prefix(h, total_a, shifts):
        for shift in shifts:
            inside = sub >= shift
            earlier_a = jnp.where(inside, pltpu.roll(total_a, shift, 0), 1.0)
            earlier_h = jnp.where(inside, pltpu.roll(h, shift, 0), 0.0)
            h = total_a * earlier_h + h
            total_a = total_a * earlier_a
        return h, total_a

    def main_slot(slot):
        for j, (a, b) in enumerate(gates(convs[slot], slot, lambda j: pace_perm[j])):
            if j == 0:
                h, total_a = b, a
            elif j == EDGE:
                h = jnp.where(sub == 0, b, a * h + b)
                total_a = jnp.where(sub == 0, a, total_a * a)
            else:
                h = a * h + b
                total_a = total_a * a
            place = slice(SUB * j, SUB * (j + 1))
            hloc[slot, place] = h
            acum[slot, place] = total_a
        h, total_a = prefix(h, total_a, (1, 2, 4))
        all_h[slot] = h
        all_a[slot] = total_a

    def conv_edge():
        own = pltpu.roll(x[:SUB, :].astype(jnp.float32), EDGE, 0)
        before = jnp.concatenate([halo[...].astype(jnp.float32)] * (SUB // CONV), axis=0)
        wide = lax.broadcasted_iota(jnp.int32, own.shape, 0)
        rows = jnp.where(wide < EDGE, before, own)
        taps = cw[...].astype(jnp.float32)
        total = taps[0:1] * rows
        for k in range(1, CONV):
            total = total + taps[k : k + 1] * pltpu.roll(rows, SUB - k, 0)
        conv0[...] = total

    def edge_slot(slot):
        (a, b), = gates(conv0[:, columns(slot)], slot, lambda j: pace_mat[:SUB, :])
        h, total_a = prefix(b, a, (1, 2))
        edge_h[slot] = h
        edge_a[slot] = total_a
        first_h = jnp.broadcast_to(h[EDGE - 1 : EDGE], (SUB, block))
        first_a = jnp.broadcast_to(total_a[EDGE - 1 : EDGE], (SUB, block))
        h, total_a = all_h[slot], all_a[slot]
        before_h = jnp.where(sub >= 1, pltpu.roll(h, 1, 0), 0.0)
        before_a = jnp.where(sub >= 1, pltpu.roll(total_a, 1, 0), 1.0)
        ex_h[slot] = before_h + before_a * first_h
        ex_a[slot] = before_a * first_a
        h = h + total_a * first_h
        log_a = jnp.log2(jnp.maximum(total_a * first_a, TINY))
        for t in range(tiles):
            lanes = slice(LANES * t, LANES * (t + 1))
            stage[pl.ds(slot * tiles + t, 1), :] = log_a[SUB - 1 :, lanes]
            stage[pl.ds(lines + slot * tiles + t, 1), :] = h[SUB - 1 :, lanes]

    with scope("meet_early"):
        meet_early()
    with scope("loads"):
        for load in loads:
            load.wait()
    last[...] = pltpu.roll(x[count - SUB :, :].astype(jnp.float32), EDGE, 0)[:CONV].astype(jnp.bfloat16)
    with scope("meet_maps"):
        meet_maps()
    with scope("maps_a"):
        for load in map_loads[:FIRST]:
            load.wait()
        for own in range(min(FIRST, hl)):
            for copy in w_copies[own::hl]:
                copy.start()

    def send_halo():
        if root > 0:

            @pl.when(me < root)
            def _():
                halo_copy.start()

    @pl.when(d > 0)
    def _():
        send_halo()

    factors[...] = softplus_neg(rate[...]) * (-gate_power / LN2)
    spread = jnp.broadcast_to(pace_row[...], (LANES, count)).T
    pace_mat[...] = spread
    for j in range(steps):
        pace_perm[j] = pace_mat[pl.ds(j, SUB, stride=steps), :]

    with scope("conv_a"):
        for slot in range(hl // 4):
            conv_main(slot)
    with scope("meet_halo"):
        meet_halo()

    @pl.when(d == 0)
    def _():
        send_halo()

    with scope("conv_b"):
        for slot in range(hl // 4, hl):
            conv_main(slot)
    with scope("maps_b"):
        for load in map_loads[FIRST:]:
            load.wait()
        for own in range(FIRST, hl):
            for copy in w_copies[own::hl]:
                copy.start()
    def wait_halo():
        with scope("take_halo"):

            @pl.when(me > 0)
            def _():
                halo_copy.wait_recv()

    def wait_maps(turn):
        with scope("map%d" % turn[0]):
            for slot in turn:
                w_copies[slot - hl].wait_recv()

    def mains(turn, after=()):
        for slot in turn:
            main_slot(slot)
        for slot in after:
            conv_main(slot)

    def edges():
        conv_edge()
        for slot in range(heads):
            edge_slot(slot)
        send_buf[...] = stage[...].astype(jnp.bfloat16)

    own, rest = list(range(hl)), list(range(hl, heads))
    pair, single = rest[:2], [[slot] for slot in rest]

    def run(turns, ahead):
        for turn, after in zip(turns, ahead):
            wait_maps(turn)
            with scope("main%d" % turn[0]):
                mains(turn, after)

    with scope("main0"):
        mains(own, pair)

    @pl.when(d == 0)
    def _():
        run(([pair] if pair else []) + single[2:], single[2:] + [[]])
        wait_halo()
        with scope("edges"):
            edges()

    @pl.when(d > 0)
    def _():
        run(single[:-1], [[]] + single[2:])
        wait_halo()
        for turn in single[-1:]:
            wait_maps(turn)
        with scope("edges"):
            for turn in single[-1:]:
                mains(turn)
            edges()

    planes = -(-nsp // ROW)
    split = reach // ROW + 1 if relay else 0
    early = jnp.logical_and(me < near, d == 0) if relay else me < 0

    def all_in():
        if root > 0:

            @pl.when(me < root)
            def _():
                pl.semaphore_wait(known.at[0], 1)

    def send_first(low, high):
        for rest in reversed(range(ROW)):
            for plane in reversed(range(low, high)):
                if 0 < ROW * plane + rest < nsp:
                    carry_copy(0, ROW * plane + rest, lines).start()

    def send_rest(low, high):
        at = lax.rem(me, ROW)
        mid = 1 - lax.rem((at + 1) // 2, 2)
        rests = (ROW - 1 - at, mid, ROW - 1 - mid, at)
        for rest, way in zip(rests, (-1, 1, 1, 1)):
            for plane in range(low, high)[::way]:
                dst = ROW * plane + rest

                @pl.when(jnp.logical_and(me < dst, dst < nsp))
                def _(dst=dst):
                    carry_copy(me, dst).start()

    def send(low, high):
        @pl.when(me == 0)
        def _():
            send_first(low, high)

        @pl.when(me > 0)
        def _():
            send_rest(low, high)

    if relay:

        @pl.when(early)
        def _():
            pl.semaphore_wait(known.at[1], 1)
            send(0, split)

    with scope("all_in"):
        all_in()

    if relay:

        @pl.when(early)
        def _():
            send(split, planes)

    @pl.when(jnp.logical_not(early))
    def _():
        send(0, planes)

    with scope("lay"):

        @pl.loop(0, heads)
        def _(slot):
            before_h, before_a = ex_h[slot], ex_a[slot]
            for j in range(steps):
                place = slice(SUB * j, SUB * (j + 1))
                h = hloc[slot, place] + acum[slot, place] * before_h
                total_a = acum[slot, place] * before_a
                if j < EDGE:
                    h = jnp.where(sub == 0, edge_h[slot, j : j + 1], h)
                    total_a = jnp.where(sub == 0, edge_a[slot, j : j + 1], total_a)
                for t in range(tiles):
                    lanes = slice(LANES * t, LANES * (t + 1))
                    lay_h[t, place] = h[:, lanes]
                    lay_a[t, place] = total_a[:, lanes]
            for t in range(tiles):
                line = lax.rem(d * hl + slot, heads) * tiles + t
                for c in range(SUB):
                    for k in range(0, steps, SUB):
                        place = slice(steps * c + k, steps * c + k + SUB)
                        part_h[line, place] = lay_h[t, pl.ds(SUB * k + c, SUB, stride=SUB), :]
                        part_a[line, place] = lay_a[t, pl.ds(SUB * k + c, SUB, stride=SUB), :]

    with scope("sent"):
        for copy in w_copies:
            copy.wait_send()

        if root > 0:

            @pl.when(me < root)
            def _():
                halo_copy.wait_send()

        for many in range(1, nsp):

            @pl.when(root - me == many)
            def _(many=many):
                carries((2 if many < root else 1) * many * lines).wait_send()

    with scope("carry"):
        for many in range(1, nsp):

            @pl.when(me == many)
            def _(many=many):
                carries((2 * many - 1) * lines).wait_recv()

    with scope("finish"):
        start = jnp.zeros(carry.shape, jnp.float32)
        parts = []
        for src in range(root):
            got = recv_buf[2 * lines * src : 2 * lines * (src + 1)].astype(jnp.float32)
            parts.append((jnp.exp2(got[:lines]), got[lines:]))
        while len(parts) > 1:
            pairs = [(a0 * a1, a1 * h0 + h1) for (a0, h0), (a1, h1) in zip(parts[::2], parts[1::2])]
            parts = pairs + parts[len(parts) // 2 * 2 :]
        if parts:
            start = parts[0][1]
        for slot in range(heads):
            line = pl.multiple_of(lax.rem(d * hl + slot, heads) * tiles, tiles)
            carry[pl.ds(line, tiles), :] = start[slot * tiles : (slot + 1) * tiles]


def finish(part_h, part_a, carry, out_hbm, out, sem):
    lines = carry.shape[0]
    count = out.shape[0]
    for low in range(0, count, 2 * SUB):
        rows = slice(low, low + 2 * SUB)
        for line in range(lines):
            state = part_h[line, rows] + part_a[line, rows] * carry[line : line + 1, :]
            out[rows, LANES * line : LANES * (line + 1)] = state.astype(jnp.bfloat16)
        pltpu.make_async_copy(out.at[rows], out_hbm.at[0, rows], sem).start()
    pltpu.make_async_copy(out, out_hbm.at[0], sem).wait()


def body(inputs, conv_weight, gate_weight, rate_param, pace):
    nsp = lax.axis_size("sp")
    ndp = lax.axis_size("dp")
    _, count, width = inputs.shape
    block = gate_weight.shape[-1]
    heads = width // block
    hl = heads // ndp
    lines = width // LANES
    f32, bf16 = jnp.float32, jnp.bfloat16
    hbm = pl.BlockSpec(memory_space=pltpu.HBM)
    dma = pltpu.SemaphoreType.DMA
    part_h, part_a, carry = pl.pallas_call(
        functools.partial(kernel, nsp, ndp, heads, block),
        out_shape=(
            pltpu.VMEM((lines, count, LANES), f32),
            pltpu.VMEM((lines, count, LANES), f32),
            pltpu.VMEM((lines, LANES), f32),
        ),
        in_specs=[hbm] * 5,
        out_specs=[pl.BlockSpec(memory_space=pltpu.VMEM)] * 3,
        scratch_shapes=[
            pltpu.VMEM((count, width), bf16),
            pltpu.VMEM(conv_weight.shape, bf16),
            pltpu.VMEM((2, heads, block, block), bf16),
            pltpu.VMEM((lines, LANES), f32),
            pltpu.VMEM((lines, LANES), f32),
            pltpu.VMEM((1, count), f32),
            pltpu.VMEM((count, LANES), f32),
            pltpu.VMEM((count // SUB, SUB, LANES), f32),
            pltpu.VMEM((CONV, width), bf16),
            pltpu.VMEM((CONV, width), bf16),
            pltpu.VMEM((heads, count, block), f32),
            pltpu.VMEM((SUB, width), f32),
            pltpu.VMEM((heads, count, block), f32),
            pltpu.VMEM((heads, count, block), f32),
            pltpu.VMEM((heads, SUB, block), f32),
            pltpu.VMEM((heads, SUB, block), f32),
            pltpu.VMEM((heads, SUB, block), f32),
            pltpu.VMEM((heads, SUB, block), f32),
            pltpu.VMEM((heads, SUB, block), f32),
            pltpu.VMEM((heads, SUB, block), f32),
            pltpu.VMEM((block // LANES, count, LANES), f32),
            pltpu.VMEM((block // LANES, count, LANES), f32),
            pltpu.VMEM((2 * lines, LANES), f32),
            pltpu.VMEM((2 * lines, LANES), bf16),
            pltpu.VMEM((2 * lines * nsp, LANES), bf16),
            pltpu.SemaphoreType.REGULAR((2,)),
            pltpu.SemaphoreType.REGULAR,
            dma,
            dma((2,)),
            dma,
            dma((heads - hl,)),
            dma,
            dma,
        ],
        compiler_params=pltpu.CompilerParams(collective_id=0, has_side_effects=True),
    )(inputs, conv_weight, gate_weight, rate_param.reshape(lines, LANES), pace)
    return pl.pallas_call(
        finish,
        out_shape=jax.ShapeDtypeStruct(inputs.shape, bf16),
        in_specs=[pl.BlockSpec(memory_space=pltpu.VMEM)] * 3,
        out_specs=hbm,
        scratch_shapes=[pltpu.VMEM((count, width), bf16), dma],
        compiler_params=pltpu.CompilerParams(vmem_limit_bytes=8 * 2**20),
    )(part_h, part_a, carry)


def solution(mesh):
    return jax.shard_map(
        body,
        mesh=mesh,
        in_specs=(P("dp", "sp", None), P(), P(None, "dp", None, None), P(), P("dp", None)),
        out_specs=P("dp", "sp", None),
        check_vma=False,
    )
```
